256 devices in a mesh: sp: 64 (over z, y, core), tp: 4 (over x).
Axes of the slice: x: 4, y: 4, z: 8, core: 2. Of those that a mesh axis runs over, the one named last changes fastest.
Arguments:
- tokens: bfloat16 [49152, 2048], P('sp', 'tp'), may hold values from -12 to 12
- query_weight: bfloat16 [2048, 1024], P('sp', 'tp'), may hold values from -0.176776695 to 0.176776695
- key_projection: bfloat16 [2048, 512], P('sp', 'tp'), may hold values from -0.176776695 to 0.176776695
- value_projection: bfloat16 [2048, 512], P('sp', 'tp'), may hold values from -0.125 to 0.125
- conv_in_weight: bfloat16 [2048, 1024], P('sp', 'tp'), may hold values from -0.125 to 0.125
- conv_gate_out: bfloat16 [2048, 1024], P('sp', 'tp'), may hold values from -0.125 to 0.125
- conv_gate_in: bfloat16 [2048, 1024], P('sp', 'tp'), may hold values from -0.125 to 0.125
- conv_taps: bfloat16 [3, 1024], P(None, 'tp'), may hold values from -3 to 3
- head_sink_logit: float32 [8], P('tp'), may hold values from 3 to 8
- out_attn_weight: bfloat16 [1024, 2048], P('tp', 'sp'), may hold values from -5 to 5
- out_conv_weight: bfloat16 [1024, 2048], P('tp', 'sp'), may hold values from -0.5 to 0.5
- out_gain: float32 [2048], P('tp'), may hold values from 0.1 to 1.9
Outputs:
- mixed: bfloat16 [49152, 2048], P('sp', 'tp')
The draws below stay inside these ranges and needn't reach their ends.
All inputs are finite; a program needn't handle non-finite values.
Results may differ from the reference program's by a relative error of at most 0.014.
Values may be sent and summed in bfloat16 or wider, within the bound.
No kernel may reach another device: no remote copies, remote signals or barrier semaphores. Data moves between devices by JAX's collectives and lax.ppermute only.
A program may use at most 64 MiB of HBM per device.

```python
import jax
import jax.numpy as jnp
from jax import lax

MODEL_WIDTH = 2048
HEAD_SIZE = 128
QUERY_HEADS = 8
KEY_VALUE_HEADS = 4
CONV = 1024
WINDOW = 128
GRID = 64
TOKENS = 49152


def draw_tokens(key, part):
    base = jnp.clip(jax.random.normal(jax.random.fold_in(key, 3), (TOKENS, MODEL_WIDTH), jnp.float32), -6.0, 6.0)
    return jnp.clip(base, -12.0, 12.0).astype(jnp.bfloat16)


def query_key_pair(key):
    head_group = QUERY_HEADS // KEY_VALUE_HEADS
    limit_value = 8.0 * MODEL_WIDTH ** (-0.5)
    query_portion = jnp.clip(jax.random.normal(jax.random.fold_in(key, 21), (MODEL_WIDTH, KEY_VALUE_HEADS, head_group, HEAD_SIZE), jnp.float32), -6.0, 6.0)
    key_portion = jnp.clip(jax.random.normal(jax.random.fold_in(key, 22), (MODEL_WIDTH, KEY_VALUE_HEADS, 1, HEAD_SIZE), jnp.float32), -6.0, 6.0)
    query_matrix = jnp.clip(query_portion.reshape(MODEL_WIDTH, QUERY_HEADS * HEAD_SIZE) * MODEL_WIDTH ** (-0.5), -limit_value, limit_value)
    key_projected = jnp.clip(key_portion.reshape(MODEL_WIDTH, KEY_VALUE_HEADS * HEAD_SIZE) * MODEL_WIDTH ** (-0.5), -limit_value, limit_value)
    return (query_matrix, key_projected)


def draw_query_weight(key, part):
    return query_key_pair(key)[0].astype(jnp.bfloat16)


def draw_key_projection(key, part):
    return query_key_pair(key)[1].astype(jnp.bfloat16)


def out_block(key, salt, rows, factor, limit):
    base = jnp.clip(jax.random.normal(jax.random.fold_in(key, salt), (rows, MODEL_WIDTH), jnp.float32), -6.0, 6.0)
    common = 0.7 * jnp.clip(jax.random.normal(jax.random.fold_in(key, salt + 1), (rows, 1), jnp.float32), -6.0, 6.0)
    column = jnp.arange(MODEL_WIDTH, dtype=jnp.int32).astype(jnp.float32) / (MODEL_WIDTH - 1)
    exponent = column - 0.5
    scale = (10.0 ** exponent)[None, :]
    value_rows = (base + common) * scale * factor * rows ** (-0.5)
    return jnp.clip(value_rows, -limit * rows ** (-0.5), limit * rows ** (-0.5)).astype(jnp.bfloat16)


def draw_out_attn_weight(key, part):
    return out_block(key, 41, QUERY_HEADS * HEAD_SIZE, 5.0, 160.0)


def draw_out_conv_weight(key, part):
    return out_block(key, 51, CONV, 0.5, 16.0)


def shard_levels(rng, dims, cuts, smallest, largest):
    def one(dim, parts):
        steps = jax.random.uniform(jax.random.fold_in(jax.random.fold_in(rng, 6), dim), (parts,), jnp.float32, smallest / len(cuts), largest / len(cuts))
        return jnp.repeat(jnp.exp(steps), dims[dim] // parts).reshape((-1,) + (1,) * (len(dims) - dim - 1))

    factor_of = one(*cuts[0])
    for cut in cuts[1:]:
        factor_of = factor_of * one(*cut)
    return factor_of


def scatter_about(stream_key, dims, scale, most, shards=(), kind=jnp.bfloat16):
    array = scale * jax.random.normal(stream_key, dims, jnp.float32)
    if shards:
        array = array * shard_levels(stream_key, dims, shards, -0.22, 0.18)
    return jnp.clip(array, -most, most).astype(kind)


def setup_inputs(seed: int = 0) -> dict:
    key_list = jax.random.split(jax.random.key(seed), 13)
    return {
        "tokens": draw_tokens(jax.random.fold_in(key_list[12], 71), 0),
        "query_weight": draw_query_weight(jax.random.fold_in(key_list[12], 71), 0),
        "key_projection": draw_key_projection(jax.random.fold_in(key_list[12], 71), 0),
        "value_projection": scatter_about(key_list[3], (MODEL_WIDTH, KEY_VALUE_HEADS * HEAD_SIZE), MODEL_WIDTH ** -0.5, 0.125, ((0, 64), (1, 4))),
        "conv_in_weight": scatter_about(key_list[4], (MODEL_WIDTH, CONV), MODEL_WIDTH ** -0.5, 0.125, ((0, 64), (1, 4))),
        "conv_gate_out": scatter_about(key_list[5], (MODEL_WIDTH, CONV), MODEL_WIDTH ** -0.5, 0.125, ((0, 64), (1, 4))),
        "conv_gate_in": scatter_about(key_list[6], (MODEL_WIDTH, CONV), MODEL_WIDTH ** -0.5, 0.125, ((0, 64), (1, 4))),
        "conv_taps": scatter_about(key_list[7], (3, CONV), 0.6, 3.0, ((1, 4),)),
        "head_sink_logit": jnp.clip(3.0 + 5.0 * jax.random.uniform(key_list[8], (QUERY_HEADS,), jnp.float32) ** shard_levels(key_list[8], (QUERY_HEADS,), ((0, 4),), -0.2, 0.2), 3.0, 8.0),
        "out_attn_weight": draw_out_attn_weight(jax.random.fold_in(key_list[12], 71), 0),
        "out_conv_weight": draw_out_conv_weight(jax.random.fold_in(key_list[12], 71), 0),
        "out_gain": jnp.clip(1.0 + 0.18 * jax.random.normal(key_list[11], (MODEL_WIDTH,), jnp.float32), 0.1, 1.9),
    }


NEG_BIG = -1e+30
THETA = 10000.0
EPS = 1e-05

def rope_tables(positions):
    row = (positions // GRID).astype(jnp.float32)
    column = (positions % GRID).astype(jnp.float32)
    half = HEAD_SIZE // 2
    inverse = THETA ** (-jnp.arange(0, half, 2, dtype=jnp.float32) / half)
    angle_row = row[:, None] * inverse
    angle_col = column[:, None] * inverse
    angles = jnp.concatenate([angle_row, angle_row, angle_col, angle_col], -1)
    return (jnp.cos(angles)[:, None, :], jnp.sin(angles)[:, None, :])

def rotate(vectors, cosine, sine):
    first, second, third, fourth = jnp.split(vectors, 4, axis=-1)
    turned = jnp.concatenate([-second, first, -fourth, third], -1)
    return vectors * cosine + turned * sine

def band_head(inputs):
    query_vectors, key_rows, value_rows, sink = inputs
    item_count = query_vectors.shape[0]
    blocks = item_count // WINDOW

    def band(block):
        padded = jnp.pad(block, ((WINDOW, WINDOW), (0, 0))).reshape(blocks + 2, WINDOW, HEAD_SIZE)
        return jnp.concatenate([padded[:-2], padded[1:-1], padded[2:]], axis=1)
    query_blocks = query_vectors.reshape(blocks, WINDOW, -1, HEAD_SIZE).astype(jnp.float32)
    key_band = band(key_rows).astype(jnp.float32)
    value_band = band(value_rows).astype(jnp.float32)
    scores = jnp.einsum('nqgd,nkd->ngqk', query_blocks, key_band) * HEAD_SIZE ** (-0.5)
    block_start = jnp.arange(blocks, dtype=jnp.int32)[:, None] * WINDOW
    query_pos = block_start + jnp.arange(WINDOW, dtype=jnp.int32)[None, :]
    key_pos = block_start - WINDOW + jnp.arange(3 * WINDOW, dtype=jnp.int32)[None, :]
    distance = key_pos[:, None, :] - query_pos[:, :, None]
    valid = (jnp.abs(distance) <= WINDOW) & (key_pos[:, None, :] >= 0) & (key_pos[:, None, :] < item_count)
    scores = jnp.where(valid[:, None], scores, NEG_BIG)
    sink_col = sink.astype(jnp.float32).reshape(1, -1, 1, 1)
    top = jnp.maximum(lax.optimization_barrier(jnp.max(scores, -1, keepdims=True)), sink_col)
    weights = jnp.exp(scores - top)
    denominator = lax.optimization_barrier(jnp.sum(weights, -1, keepdims=True)) + jnp.exp(sink_col - top)
    probs = lax.optimization_barrier((weights / denominator).astype(jnp.bfloat16)).astype(jnp.float32)
    mixed = jnp.einsum('ngqk,nkd->nqgd', probs, value_band)
    return mixed.reshape(item_count, -1, HEAD_SIZE).astype(jnp.bfloat16)

def reference(tokens, query_weight, key_projection, value_projection, conv_in_weight, conv_gate_out, conv_gate_in, conv_taps, head_sink_logit, out_attn_weight, out_conv_weight, out_gain):
    item_count = tokens.shape[0]
    head_group = QUERY_HEADS // KEY_VALUE_HEADS
    positions = jnp.arange(item_count, dtype=jnp.int32)
    cosine, sine = rope_tables(positions)
    query_raw = jnp.dot(tokens, query_weight, preferred_element_type=jnp.float32).reshape(item_count, QUERY_HEADS, HEAD_SIZE)
    query_vectors = rotate(query_raw, cosine, sine).astype(jnp.bfloat16)
    key_unrotated = jnp.dot(tokens, key_projection, preferred_element_type=jnp.float32).reshape(item_count, KEY_VALUE_HEADS, HEAD_SIZE)
    key_rows = rotate(key_unrotated, cosine, sine).astype(jnp.bfloat16)
    value_rows = jnp.dot(tokens, value_projection, preferred_element_type=jnp.float32).astype(jnp.bfloat16)
    value_rows = value_rows.reshape(item_count, KEY_VALUE_HEADS, HEAD_SIZE)
    head_major = (jnp.transpose(query_vectors.reshape(item_count, KEY_VALUE_HEADS, head_group, HEAD_SIZE), (1, 0, 2, 3)), jnp.transpose(key_rows, (1, 0, 2)), jnp.transpose(value_rows, (1, 0, 2)), head_sink_logit.reshape(KEY_VALUE_HEADS, head_group))
    mixed_heads = lax.map(band_head, head_major)
    attention_out = jnp.transpose(mixed_heads, (1, 0, 2, 3)).reshape(item_count, QUERY_HEADS * HEAD_SIZE)
    conv_input = jnp.dot(tokens, conv_in_weight, preferred_element_type=jnp.float32)
    gate_after = jnp.dot(tokens, conv_gate_out, preferred_element_type=jnp.float32)
    gate_before = jnp.dot(tokens, conv_gate_in, preferred_element_type=jnp.float32)
    sectioned = (gate_before * conv_input).astype(jnp.bfloat16)
    padded = jnp.pad(sectioned, ((1, 1), (0, 0))).astype(jnp.float32)
    taps = conv_taps.astype(jnp.float32)
    conv_mix = padded[:-2] * taps[0] + padded[1:-1] * taps[1] + padded[2:] * taps[2]
    conv_out = (gate_after * conv_mix).astype(jnp.bfloat16)
    summed = jnp.dot(attention_out, out_attn_weight, preferred_element_type=jnp.float32) + jnp.dot(conv_out, out_conv_weight, preferred_element_type=jnp.float32)
    mean = lax.optimization_barrier(jnp.mean(summed, -1, keepdims=True))
    spread = lax.optimization_barrier(jnp.mean(jnp.square(summed - mean), -1, keepdims=True))
    return ((summed - mean) * lax.rsqrt(spread + EPS) * out_gain).astype(jnp.bfloat16)
```

```python
import functools

import jax
import jax.numpy as jnp
from jax import lax
from jax.experimental import pallas as pl
from jax.experimental.pallas import tpu as pltpu
from jax.sharding import PartitionSpec as P

HEAD = 128
WINDOW = 128
GRID = 64
NEG_BIG = -1e30
THETA = 10000.0
EPS = 1e-05

ROWS = 768
EXT = ROWS + 2 * WINDOW
WIDTH = 2048
PART = 512
QKV = 512
CNV = 768
OUT = 512
ZB = 256


ANY = pl.BlockSpec(memory_space=pl.ANY)
SMEM = pl.BlockSpec(memory_space=pltpu.SMEM)
VMEM = pl.BlockSpec(memory_space=pltpu.VMEM)
F32 = jnp.float32
BF16 = jnp.bfloat16


def chip(z, y, c):
    return ((z % 8) * 4 + y % 4) * 2 + c


def up_down():
    return [
        (chip(z, y, c), chip(z + 1 - 2 * c, y, c))
        for z in range(8)
        for y in range(4)
        for c in range(2)
    ]


def partner():
    return [(i, i ^ 1) for i in range(64)]


def turn(d):
    return [(i, (i + d) % 4) for i in range(4)]


def spread_out_weights():
    pairs = []
    for z in range(8):
        for y in range(4):
            for c in range(2):
                for t in range(4):
                    target = chip((z % 2) * 4 + t, y, c) * 4 + z // 2
                    pairs.append((chip(z, y, c) * 4 + t, target))
    return pairs


def x_ring(block):
    h = block.shape[0] // 2
    r1 = lax.ppermute(block, "tp", turn(1))
    l1 = lax.ppermute(block, "tp", turn(-1))
    r2 = lax.ppermute(r1[:h], "tp", turn(1))
    l2 = lax.ppermute(l1[h:], "tp", turn(-1))
    return [block, r1, l1, r2, l2]


def z_ring(block):
    m1 = lax.ppermute(block, "sp", up_down())
    m2 = lax.ppermute(m1, "sp", up_down())
    m3 = lax.ppermute(m2, "sp", up_down())
    m4 = lax.ppermute(m3, "sp", up_down())
    e = lax.ppermute(jnp.concatenate([m1, m2, m3], 0), "sp", partner())
    return [block, m1, m2, m3, m4, e]


def fetch(copies):
    for c in copies:
        c.start()
    for c in copies:
        c.wait()


def token_copies(sc, toks, tb, sem):
    own, r1, l1, r2, l2 = toks
    h = own.shape[0] // 2
    at = [pl.multiple_of(sc[8 + i] * PART, PART) for i in range(4)]
    return [
        pltpu.make_async_copy(own, tb.at[:, pl.ds(at[0], PART)], sem.at[0]),
        pltpu.make_async_copy(r1, tb.at[:, pl.ds(at[1], PART)], sem.at[1]),
        pltpu.make_async_copy(l1, tb.at[:, pl.ds(at[2], PART)], sem.at[2]),
        pltpu.make_async_copy(r2, tb.at[pl.ds(0, h), pl.ds(at[3], PART)], sem.at[3]),
        pltpu.make_async_copy(l2, tb.at[pl.ds(h, h), pl.ds(at[3], PART)], sem.at[4]),
    ]


def weight_sources(ws):
    block, m1, m2, m3, m4, e = ws
    return [block, m1, m2, m3, m4] + [e.at[pl.ds(k * ZB, ZB), :] for k in range(3)]


def weight_copies(sc, ws, wb, sem, base):
    out = []
    for k, src in enumerate(weight_sources(ws)):
        row = pl.multiple_of(sc[k] * ZB, ZB)
        out.append(pltpu.make_async_copy(src, wb.at[pl.ds(row, ZB), :], sem.at[base + k]))
    return out


def rotate(u, cos, sin, even):
    turned = jnp.where(even, -pltpu.roll(u, 96, 1), pltpu.roll(u, 32, 1))
    return u * cos + turned * sin


def attn_kernel(sc, sink, *refs):
    toks, ws = refs[:5], refs[5:11]
    cos_ref, sin_ref, out_ref, tb, wb, kb, vb, qb, sem = refs[11:]
    fetch(token_copies(sc, toks, tb, sem) + weight_copies(sc, ws, wb, sem, 5))
    even = (lax.broadcasted_iota(jnp.int32, (256, HEAD), 1) // 32) % 2 == 0

    def keys(i, _):
        r = pl.multiple_of(i * 256, 256)
        rows = pl.ds(r, 256)
        kv = jnp.dot(tb[rows, :], wb[:, :256], preferred_element_type=F32)
        kb[rows, :] = rotate(kv[:, :HEAD], cos_ref[rows, :], sin_ref[rows, :], even).astype(BF16)
        vb[rows, :] = kv[:, HEAD:].astype(BF16)
        return 0

    lax.fori_loop(0, EXT // 256, keys, 0)

    def queries(i, _):
        r = pl.multiple_of(i * 256, 256)
        rows = pl.ds(pl.multiple_of(r + WINDOW, WINDOW), 256)
        q = jnp.dot(tb[rows, :], wb[:, 256:], preferred_element_type=F32)
        cos, sin = cos_ref[rows, :], sin_ref[rows, :]
        for h in range(2):
            part = rotate(q[:, h * HEAD : (h + 1) * HEAD], cos, sin, even)
            qb[pl.ds(r, 256), h * HEAD : (h + 1) * HEAD] = part.astype(BF16)
        return 0

    lax.fori_loop(0, ROWS // 256, queries, 0)

    place = sc[12]
    row = lax.broadcasted_iota(jnp.int32, (WINDOW, 3 * WINDOW), 0)
    col = lax.broadcasted_iota(jnp.int32, (WINDOW, 3 * WINDOW), 1)
    near = (col >= row) & (col <= row + 2 * WINDOW)

    def block(n, _):
        r = pl.multiple_of(n * WINDOW, WINDOW)
        low = jnp.where((place == 0) & (n == 0), WINDOW, 0)
        high = jnp.where((place == 63) & (n == ROWS // WINDOW - 1), 2 * WINDOW, 3 * WINDOW)
        valid = near & (col >= low) & (col < high)
        k = kb[pl.ds(r, 3 * WINDOW), :]
        v = vb[pl.ds(r, 3 * WINDOW), :]
        for h in range(2):
            lanes = slice(h * HEAD, (h + 1) * HEAD)
            q = qb[pl.ds(r, WINDOW), lanes]
            s = lax.dot_general(q, k, (((1,), (1,)), ((), ())), preferred_element_type=F32)
            s = jnp.where(valid, s * HEAD ** (-0.5), NEG_BIG)
            top = jnp.maximum(jnp.max(s, -1, keepdims=True), sink[h])
            w = jnp.exp(s - top)
            total = jnp.sum(w, -1, keepdims=True) + jnp.exp(sink[h] - top)
            probs = (w / total).astype(BF16)
            o = jnp.dot(probs, v, preferred_element_type=F32)
            out_ref[pl.ds(r, WINDOW), lanes] = o.astype(BF16)
        return 0

    lax.fori_loop(0, ROWS // WINDOW, block, 0)


CONV_ROWS = ROWS + 32


def conv_kernel(sc, *refs):
    toks, ws = refs[:5], refs[5:11]
    taps_ref, out_ref, tb, wb, sb, sem = refs[11:]
    fetch(token_copies(sc, toks, tb, sem) + weight_copies(sc, ws, wb, sem, 5))

    def section(i, _):
        r = pl.multiple_of(i * 160, 160)
        rows = pl.ds(pl.multiple_of(r + 112, 16), 160)
        both = jnp.dot(tb[rows, :], wb[:, :512], preferred_element_type=F32)
        sb[pl.ds(r, 160), :] = (both[:, 256:] * both[:, :256]).astype(BF16).astype(F32)
        return 0

    lax.fori_loop(0, CONV_ROWS // 160, section, 0)
    taps = taps_ref[...].astype(F32)

    def mix(i, _):
        r = pl.multiple_of(i * 256, 256)
        rows = pl.ds(pl.multiple_of(r + WINDOW, WINDOW), 256)
        gate = jnp.dot(tb[rows, :], wb[:, 512:], preferred_element_type=F32)
        s = sb[pl.ds(pl.multiple_of(r + 8, 8), 272), :]
        before = pltpu.roll(s, 1, 0)[8:264]
        after = pltpu.roll(s, 271, 0)[8:264]
        conv = before * taps[0:1] + s[8:264] * taps[1:2] + after * taps[2:3]
        out_ref[pl.ds(r, 256), :] = (gate * conv).astype(BF16)
        return 0

    lax.fori_loop(0, ROWS // 256, mix, 0)


def out_kernel(sc, *refs):
    attn, conv, ws = refs[:5], refs[5:10], refs[10:16]
    out_ref, stat_ref, mb, wb, sem = refs[16:]
    h = ROWS // 2
    copies = []
    for j, pieces in enumerate((attn, conv)):
        own, r1, l1, r2, l2 = pieces
        at = [pl.multiple_of(sc[8 + i] * PART + j * 256, 256) for i in range(4)]
        spots = [
            (own, mb.at[:, pl.ds(at[0], 256)]),
            (r1, mb.at[:, pl.ds(at[1], 256)]),
            (l1, mb.at[:, pl.ds(at[2], 256)]),
            (r2, mb.at[pl.ds(0, h), pl.ds(at[3], 256)]),
            (l2, mb.at[pl.ds(h, h), pl.ds(at[3], 256)]),
        ]
        for i, (src, dst) in enumerate(spots):
            copies.append(pltpu.make_async_copy(src, dst, sem.at[j * 5 + i]))
    for k, src in enumerate(weight_sources(ws)):
        row = pl.multiple_of((sc[k] // 4) * ZB, ZB)
        lane = pl.multiple_of((sc[k] % 4) * PART, PART)
        copies.append(
            pltpu.make_async_copy(src, wb.at[pl.ds(row, ZB), pl.ds(lane, PART)], sem.at[10 + k])
        )
    fetch(copies)

    def rows_of(i, _):
        r = pl.multiple_of(i * 128, 128)
        rows = pl.ds(r, 128)
        s = lax.dot_general(
            mb[rows, :], wb[...], (((1,), (1,)), ((), ())), preferred_element_type=F32
        )
        out_ref[rows, :] = s
        mean = jnp.sum(s, -1, keepdims=True) * (1.0 / PART)
        d = s - mean
        second = jnp.sum(d * d, -1, keepdims=True)
        stat_ref[0:1, rows] = jnp.broadcast_to(mean, (128, 128)).T[0:1]
        stat_ref[1:2, rows] = jnp.broadcast_to(second, (128, 128)).T[0:1]
        return 0

    lax.fori_loop(0, ROWS // 128, rows_of, 0)


def norm_kernel(sum_ref, s0, s1, s2, s3, gain_ref, out_ref):
    parts = (s0, s1, s2, s3)
    gain = gain_ref[...]

    def rows_of(i, _):
        r = pl.multiple_of(i * 128, 128)
        rows = pl.ds(r, 128)
        means = [p[0:1, rows] for p in parts]
        mean = (means[0] + means[1] + means[2] + means[3]) * 0.25
        second = sum(p[1:2, rows] for p in parts)
        second = second + PART * sum((m - mean) * (m - mean) for m in means)
        scale = lax.rsqrt(second * (1.0 / WIDTH) + EPS)
        mean = jnp.broadcast_to(mean, (128, 128)).T[:, 0:1]
        scale = jnp.broadcast_to(scale, (128, 128)).T[:, 0:1]
        out_ref[rows, :] = ((sum_ref[rows, :] - mean) * scale * gain).astype(BF16)
        return 0

    lax.fori_loop(0, ROWS // 128, rows_of, 0)


def pack_kernel(*refs):
    out = refs[-1]
    at = 0
    for r in refs[:-1]:
        out[:, at : at + r.shape[1]] = r[...]
        at += r.shape[1]


def cost(flops, read):
    return pl.CostEstimate(flops=int(flops), bytes_accessed=int(read), transcendentals=0)


def params():
    return pltpu.CompilerParams(vmem_limit_bytes=40 * 1024 * 1024)


def rope_tables(positions):
    row = (positions // GRID).astype(F32)
    column = (positions % GRID).astype(F32)
    half = HEAD // 2
    inverse = THETA ** (-jnp.arange(0, half, 2, dtype=F32) / half)
    angle_row = row[:, None] * inverse
    angle_col = column[:, None] * inverse
    angles = jnp.concatenate([angle_row, angle_row, angle_col, angle_col], -1)
    return jnp.cos(angles), jnp.sin(angles)


def body(
    tokens,
    query_weight,
    key_projection,
    value_projection,
    conv_in_weight,
    conv_gate_out,
    conv_gate_in,
    conv_taps,
    head_sink_logit,
    out_attn_weight,
    out_conv_weight,
    out_gain,
):
    s = lax.axis_index("sp")
    x = lax.axis_index("tp")
    z, core = s // 8, s % 2
    sign = 2 * core - 1
    steps = jnp.array([0, 1, 2, 3, 4, -1, -2, -3], jnp.int32)
    turns = jnp.array([0, -1, 1, 2], jnp.int32)
    sc = jnp.concatenate(
        [(z + sign * steps + 8) % 8, (x + turns + 4) % 4, jnp.full((4,), s, jnp.int32)]
    ).astype(jnp.int32)

    stacked = jnp.concatenate([out_attn_weight.T, out_conv_weight.T], 1)
    stacked = lax.ppermute(stacked, ("sp", "tp"), spread_out_weights())
    low = lax.ppermute(tokens[-WINDOW:], "sp", [(i, i + 1) for i in range(63)])
    high = lax.ppermute(tokens[:WINDOW], "sp", [(i + 1, i) for i in range(63)])
    ext = jnp.concatenate([low, tokens, high], 0)
    toks = x_ring(ext)

    packed = pl.pallas_call(
        pack_kernel,
        out_shape=jax.ShapeDtypeStruct((32, QKV + CNV + OUT), BF16),
        in_specs=[VMEM] * 7,
        out_specs=VMEM,
        cost_estimate=cost(1e6, 3e5),
    )(
        key_projection,
        value_projection,
        query_weight,
        conv_in_weight,
        conv_gate_in,
        conv_gate_out,
        stacked,
    )
    planes = [[chip(z, y, c) for y in range(4) for c in range(2)] for z in range(8)]
    plane = lax.all_gather(packed, "sp", axis=0, tiled=True, axis_index_groups=planes)
    w_qkv = z_ring(plane[:, :QKV])
    w_cnv = z_ring(plane[:, QKV : QKV + CNV])
    w_out = z_ring(plane[:, QKV + CNV :])

    positions = s * ROWS - WINDOW + jnp.arange(EXT, dtype=jnp.int32)
    cosine, sine = rope_tables(positions)

    attention = pl.pallas_call(
        attn_kernel,
        out_shape=jax.ShapeDtypeStruct((ROWS, 256), BF16),
        in_specs=[SMEM, SMEM] + [ANY] * 11 + [VMEM] * 2,
        out_specs=VMEM,
        scratch_shapes=[
            pltpu.VMEM((EXT, WIDTH), BF16),
            pltpu.VMEM((WIDTH, QKV), BF16),
            pltpu.VMEM((EXT, HEAD), BF16),
            pltpu.VMEM((EXT, HEAD), BF16),
            pltpu.VMEM((ROWS, 2 * HEAD), BF16),
            pltpu.SemaphoreType.DMA((13,)),
        ],
        compiler_params=params(),
        cost_estimate=cost(3.5e9, 8e6),
    )(sc, head_sink_logit, *toks, *w_qkv, cosine, sine)
    conv = pl.pallas_call(
        conv_kernel,
        out_shape=jax.ShapeDtypeStruct((ROWS, 256), BF16),
        in_specs=[SMEM] + [ANY] * 11 + [VMEM],
        out_specs=VMEM,
        scratch_shapes=[
            pltpu.VMEM((EXT, WIDTH), BF16),
            pltpu.VMEM((WIDTH, CNV), BF16),
            pltpu.VMEM((CONV_ROWS, 256), F32),
            pltpu.SemaphoreType.DMA((13,)),
        ],
        compiler_params=params(),
        cost_estimate=cost(3e9, 8e6),
    )(sc, *toks, *w_cnv, conv_taps)
    attn_all = x_ring(attention)
    conv_all = x_ring(conv)
    summed, stats = pl.pallas_call(
        out_kernel,
        out_shape=(
            jax.ShapeDtypeStruct((ROWS, PART), F32),
            jax.ShapeDtypeStruct((8, ROWS), F32),
        ),
        in_specs=[SMEM] + [ANY] * 16,
        out_specs=(VMEM, VMEM),
        scratch_shapes=[
            pltpu.VMEM((ROWS, WIDTH), BF16),
            pltpu.VMEM((PART, WIDTH), BF16),
            pltpu.SemaphoreType.DMA((18,)),
        ],
        compiler_params=params(),
        cost_estimate=cost(1.6e9, 6e6),
    )(sc, *attn_all, *conv_all, *w_out)
    others = [lax.ppermute(stats, "tp", turn(d)) for d in (1, -1, 2)]
    return pl.pallas_call(
        norm_kernel,
        out_shape=jax.ShapeDtypeStruct((ROWS, PART), BF16),
        in_specs=[VMEM] * 6,
        out_specs=VMEM,
        compiler_params=params(),
        cost_estimate=cost(4e6, 3e6),
    )(summed, stats, *others, out_gain.reshape(1, PART))


def solution(mesh):
    return jax.shard_map(
        body,
        mesh=mesh,
        in_specs=(
            P("sp", "tp"),
            P("sp", "tp"),
            P("sp", "tp"),
            P("sp", "tp"),
            P("sp", "tp"),
            P("sp", "tp"),
            P("sp", "tp"),
            P(None, "tp"),
            P("tp"),
            P("tp", "sp"),
            P("tp", "sp"),
            P("tp"),
        ),
        out_specs=P("sp", "tp"),
        check_vma=False,
    )
```

```python
import jax
import jax.numpy as jnp
from jax import lax
from jax.experimental import pallas as pl
from jax.experimental.pallas import tpu as pltpu
from jax.sharding import PartitionSpec as P


HEAD = 128
WINDOW = 128
GRID = 64
NEG_BIG = -1e30
THETA = 10000.0
EPS = 1e-05

ROWS = 768
WIDTH = 2048
PART = 512
QKV = 512
CNV = 768
OUT = 512
ZB = 256


ANY = pl.BlockSpec(memory_space=pl.ANY)
SMEM = pl.BlockSpec(memory_space=pltpu.SMEM)
VMEM = pl.BlockSpec(memory_space=pltpu.VMEM)
F32 = jnp.float32
BF16 = jnp.bfloat16


def chip(z, y, c):
    return ((z % 8) * 4 + y % 4) * 2 + c


def up_down():
    return [
        (chip(z, y, c), chip(z + 1 - 2 * c, y, c))
        for z in range(8)
        for y in range(4)
        for c in range(2)
    ]


def partner():
    return [(i, i ^ 1) for i in range(64)]


def turn(d):
    return [(i, (i + d) % 4) for i in range(4)]


def spread_out_weights():
    pairs = []
    for z in range(8):
        for y in range(4):
            for c in range(2):
                for t in range(4):
                    target = chip((z % 2) * 4 + t, y, c) * 4 + z // 2
                    pairs.append((chip(z, y, c) * 4 + t, target))
    return pairs


def x_ring(block):
    h = block.shape[0] // 2
    r1 = lax.ppermute(block, "tp", turn(1))
    l1 = lax.ppermute(block, "tp", turn(-1))
    r2 = lax.ppermute(r1[:h], "tp", turn(1))
    l2 = lax.ppermute(l1[h:], "tp", turn(-1))
    return [block, r1, l1, r2, l2]


def z_ring(block):
    got = [block]
    for _ in range(1, 5):
        got.append(lax.ppermute(got[-1], "sp", up_down()))
    e = lax.ppermute(jnp.concatenate(got[1:4], 0), "sp", partner())
    return got + [e]


def fetch(copies):
    for c in copies:
        c.start()
    for c in copies:
        c.wait()


def token_copies(sc, toks, tb, sem, top):
    own, r1, l1, r2, l2 = toks
    h = ROWS // 2
    at = [pl.multiple_of(sc[8 + i] * PART, PART) for i in range(4)]
    every = pl.ds(top, ROWS)
    spots = [
        (own, tb.at[every, pl.ds(at[0], PART)]),
        (r1, tb.at[every, pl.ds(at[1], PART)]),
        (l1, tb.at[every, pl.ds(at[2], PART)]),
        (r2, tb.at[pl.ds(top, h), pl.ds(at[3], PART)]),
        (l2, tb.at[pl.ds(top + h, h), pl.ds(at[3], PART)]),
    ]
    return [pltpu.make_async_copy(a, b, sem.at[i]) for i, (a, b) in enumerate(spots)]


def weight_sources(ws):
    block, m1, m2, m3, m4, e = ws
    return [block, m1, m2, m3, m4] + [e.at[pl.ds(k * ZB, ZB), :] for k in range(3)]


def weight_copies(sc, ws, wb, sem, base):
    out = []
    for k, src in enumerate(weight_sources(ws)):
        row = pl.multiple_of(sc[k] * ZB, ZB)
        out.append(pltpu.make_async_copy(src, wb.at[pl.ds(row, ZB), :], sem.at[base + k]))
    return out


def rotate(u, cos, sin, even):
    turned = jnp.where(even, -pltpu.roll(u, 96, 1), pltpu.roll(u, 32, 1))
    return u * cos + turned * sin


def project_kernel(sc, *refs):
    toks, ws = refs[:5], refs[5:11]
    cos_ref, sin_ref, kv_ref, q_ref, first_ref, last_ref, tb, wb, sem = refs[11:]
    fetch(token_copies(sc, toks, tb, sem, 0) + weight_copies(sc, ws, wb, sem, 5))
    n = 256
    even = (lax.broadcasted_iota(jnp.int32, (n, HEAD), 1) // 32) % 2 == 0
    for i in range(ROWS // n):
        rows = slice(i * n, (i + 1) * n)
        u = jnp.dot(tb[rows, :], wb[...], preferred_element_type=F32)
        cos, sin = cos_ref[rows, :], sin_ref[rows, :]
        kv_ref[rows, :HEAD] = rotate(u[:, :HEAD], cos, sin, even).astype(BF16)
        kv_ref[rows, HEAD:] = u[:, HEAD : 2 * HEAD].astype(BF16)
        for h in range(2):
            part = u[:, (2 + h) * HEAD : (3 + h) * HEAD]
            q_ref[rows, h * HEAD : (h + 1) * HEAD] = rotate(part, cos, sin, even).astype(BF16)
    first_ref[...] = kv_ref[:WINDOW, :]
    last_ref[...] = kv_ref[ROWS - WINDOW :, :]


def attn_kernel(sc, sink, kv_ref, q_ref, low_ref, high_ref, out_ref, kb):
    kb[:WINDOW, :] = low_ref[...]
    kb[WINDOW : WINDOW + ROWS, :] = kv_ref[...]
    kb[WINDOW + ROWS :, :] = high_ref[...]
    place = sc[12]
    two = 2 * WINDOW
    row = lax.broadcasted_iota(jnp.int32, (two, WINDOW), 0) % WINDOW
    col = lax.broadcasted_iota(jnp.int32, (two, WINDOW), 1)
    sinks = jnp.where(
        lax.broadcasted_iota(jnp.int32, (two, 1), 0) < WINDOW, sink[0], sink[1]
    )
    count = ROWS // WINDOW
    for n in range(count):
        left, right = col >= row, col <= row
        if n == 0:
            left = left & (col >= jnp.where(place == 0, WINDOW, 0))
        if n == count - 1:
            right = right & (col < jnp.where(place == 63, 0, WINDOW))
        keys = slice(n * WINDOW, (n + 3) * WINDOW)
        rows = slice(n * WINDOW, (n + 1) * WINDOW)
        k, v = kb[keys, :HEAD], kb[keys, HEAD:]
        q = jnp.concatenate([q_ref[rows, :HEAD], q_ref[rows, HEAD:]], 0)
        s = lax.dot_general(q, k, (((1,), (1,)), ((), ())), preferred_element_type=F32)
        s = s * HEAD ** (-0.5)
        s0 = jnp.where(left, s[:, :WINDOW], NEG_BIG)
        s1 = s[:, WINDOW:two]
        s2 = jnp.where(right, s[:, two:], NEG_BIG)
        top = jnp.maximum(jnp.maximum(s0, s1), s2)
        top = jnp.maximum(jnp.max(top, -1, keepdims=True), sinks)
        w0, w1, w2 = jnp.exp(s0 - top), jnp.exp(s1 - top), jnp.exp(s2 - top)
        total = jnp.sum(w0 + w1 + w2, -1, keepdims=True) + jnp.exp(sinks - top)
        inverse = 1.0 / total
        probs = jnp.concatenate([w0 * inverse, w1 * inverse, w2 * inverse], 1).astype(BF16)
        o = jnp.dot(probs, v, preferred_element_type=F32).astype(BF16)
        out_ref[rows, :HEAD] = o[:WINDOW]
        out_ref[rows, HEAD:] = o[WINDOW:]


CONV_ROWS = ROWS + 32


def conv_kernel(sc, *refs):
    toks, ws = refs[:5], refs[5:11]
    low_ref, high_ref, taps_ref, out_ref, tb, wb, sb, sem = refs[11:]
    copies = token_copies(sc, toks, tb, sem, 16) + weight_copies(sc, ws, wb, sem, 5)
    for c in copies:
        c.start()
    for i in range(4):
        lanes = pl.ds(pl.multiple_of(sc[8 + i] * PART, PART), PART)
        tb[:16, lanes] = low_ref[:, i * PART : i * PART + PART]
        tb[16 + ROWS :, lanes] = high_ref[:, i * PART : i * PART + PART]
    for c in copies:
        c.wait()
    for lo, hi in ((0, 272), (272, 544), (544, 800)):
        both = jnp.dot(tb[lo:hi, :], wb[:, :512], preferred_element_type=F32)
        sb[lo:hi, :] = (both[:, 256:] * both[:, :256]).astype(BF16).astype(F32)
    taps = taps_ref[...].astype(F32)
    for i in range(ROWS // 256):
        r = i * 256
        gate = jnp.dot(tb[16 + r : 272 + r, :], wb[:, 512:], preferred_element_type=F32)
        s = sb[r + 8 : r + 280, :]
        before = pltpu.roll(s, 1, 0)[8:264]
        after = pltpu.roll(s, 271, 0)[8:264]
        conv = before * taps[0:1] + s[8:264] * taps[1:2] + after * taps[2:3]
        out_ref[r : r + 256, :] = (gate * conv).astype(BF16)


def out_kernel(sc, *refs):
    attn, conv, ws = refs[:5], refs[5:10], refs[10:16]
    out_ref, stat_ref, mb, wb, sem = refs[16:]
    h = ROWS // 2
    copies = []
    for j, pieces in enumerate((attn, conv)):
        own, r1, l1, r2, l2 = pieces
        at = [pl.multiple_of(sc[8 + i] * PART + j * 256, 256) for i in range(4)]
        spots = [
            (own, mb.at[:, pl.ds(at[0], 256)]),
            (r1, mb.at[:, pl.ds(at[1], 256)]),
            (l1, mb.at[:, pl.ds(at[2], 256)]),
            (r2, mb.at[pl.ds(0, h), pl.ds(at[3], 256)]),
            (l2, mb.at[pl.ds(h, h), pl.ds(at[3], 256)]),
        ]
        for i, (src, dst) in enumerate(spots):
            copies.append(pltpu.make_async_copy(src, dst, sem.at[j * 5 + i]))
    for k, src in enumerate(weight_sources(ws)):
        row = pl.multiple_of((sc[k] // 4) * ZB, ZB)
        lane = pl.multiple_of((sc[k] % 4) * PART, PART)
        copies.append(
            pltpu.make_async_copy(src, wb.at[pl.ds(row, ZB), pl.ds(lane, PART)], sem.at[10 + k])
        )
    fetch(copies)

    for i in range(ROWS // 256):
        s = lax.dot_general(
            mb[i * 256 : i * 256 + 256, :],
            wb[...],
            (((1,), (1,)), ((), ())),
            preferred_element_type=F32,
        )
        out_ref[i * 256 : i * 256 + 256, :] = s
        mean = jnp.sum(s, -1, keepdims=True) * (1.0 / PART)
        d = s - mean
        second = jnp.sum(d * d, -1, keepdims=True)
        for j in range(2):
            part = slice(j * 128, j * 128 + 128)
            rows = slice(i * 256 + j * 128, i * 256 + j * 128 + 128)
            stat_ref[0:1, rows] = jnp.broadcast_to(mean[part], (128, 128)).T[0:1]
            stat_ref[1:2, rows] = jnp.broadcast_to(second[part], (128, 128)).T[0:1]


def norm_kernel(sum_ref, s0, s1, s2, s3, gain_ref, out_ref):
    parts = (s0, s1, s2, s3)
    gain = gain_ref[...]

    def rows_of(i, _):
        r = pl.multiple_of(i * 128, 128)
        rows = pl.ds(r, 128)
        means = [p[0:1, rows] for p in parts]
        mean = (means[0] + means[1] + means[2] + means[3]) * 0.25
        second = sum(p[1:2, rows] for p in parts)
        second = second + PART * sum((m - mean) * (m - mean) for m in means)
        scale = lax.rsqrt(second * (1.0 / WIDTH) + EPS)
        mean = jnp.broadcast_to(mean, (128, 128)).T[:, 0:1]
        scale = jnp.broadcast_to(scale, (128, 128)).T[:, 0:1]
        out_ref[rows, :] = ((sum_ref[rows, :] - mean) * scale * gain).astype(BF16)
        return 0

    lax.fori_loop(0, ROWS // 128, rows_of, 0)


def pack_kernel(*refs):
    out = refs[-1]
    at = 0
    for r in refs[:-1]:
        out[:, at : at + r.shape[1]] = r[...]
        at += r.shape[1]


def cost(flops, read):
    return pl.CostEstimate(flops=int(flops), bytes_accessed=int(read), transcendentals=0)


def params(mib):
    return pltpu.CompilerParams(vmem_limit_bytes=mib * 1024 * 1024)


def rope_tables(positions):
    row = (positions // GRID).astype(F32)
    column = (positions % GRID).astype(F32)
    half = HEAD // 2
    inverse = THETA ** (-jnp.arange(0, half, 2, dtype=F32) / half)
    angle_row = row[:, None] * inverse
    angle_col = column[:, None] * inverse
    angles = jnp.concatenate([angle_row, angle_row, angle_col, angle_col], -1)
    return jnp.cos(angles), jnp.sin(angles)


def body(
    tokens,
    query_weight,
    key_projection,
    value_projection,
    conv_in_weight,
    conv_gate_out,
    conv_gate_in,
    conv_taps,
    head_sink_logit,
    out_attn_weight,
    out_conv_weight,
    out_gain,
):
    s = lax.axis_index("sp")
    x = lax.axis_index("tp")
    z, core = s // 8, s % 2
    sign = 2 * core - 1
    steps = jnp.array([0, 1, 2, 3, 4, -1, -2, -3], jnp.int32)
    turns = jnp.array([0, -1, 1, 2], jnp.int32)
    sc = jnp.concatenate(
        [(z + sign * steps + 8) % 8, (x + turns + 4) % 4, jnp.full((4,), s, jnp.int32)]
    ).astype(jnp.int32)

    toks = x_ring(tokens)
    own, r1, l1, r2, l2 = toks
    begin = jnp.concatenate([own[:16], r1[:16], l1[:16], r2[:16]], 1)
    end = jnp.concatenate([own[-16:], r1[-16:], l1[-16:], l2[-16:]], 1)
    up = [(i, i + 1) for i in range(63)]
    down = [(i + 1, i) for i in range(63)]
    before = lax.ppermute(end, "sp", up)
    after = lax.ppermute(begin, "sp", down)

    packed = pl.pallas_call(
        pack_kernel,
        out_shape=jax.ShapeDtypeStruct((32, QKV + CNV + OUT), BF16),
        in_specs=[VMEM] * 8,
        out_specs=VMEM,
        cost_estimate=cost(1e6, 3e5),
    )(
        key_projection,
        value_projection,
        query_weight,
        conv_in_weight,
        conv_gate_in,
        conv_gate_out,
        out_attn_weight.T,
        out_conv_weight.T,
    )
    planes = [[chip(z, y, c) for y in range(4) for c in range(2)] for z in range(8)]
    plane = lax.all_gather(packed, "sp", axis=0, tiled=True, axis_index_groups=planes)
    w_qkv = z_ring(plane[:, :QKV])
    w_cnv = z_ring(plane[:, QKV : QKV + CNV])
    own_out = lax.ppermute(plane[:, QKV + CNV :], ("sp", "tp"), spread_out_weights())
    w_out = z_ring(own_out)

    positions = s * ROWS + jnp.arange(ROWS, dtype=jnp.int32)
    cosine, sine = rope_tables(positions)

    edge = jax.ShapeDtypeStruct((WINDOW, 256), BF16)
    mixer = jax.ShapeDtypeStruct((ROWS, 256), BF16)
    kv, query, first, last = pl.pallas_call(
        project_kernel,
        out_shape=(mixer, mixer, edge, edge),
        in_specs=[SMEM] + [ANY] * 11 + [VMEM] * 2,
        out_specs=(VMEM,) * 4,
        scratch_shapes=[
            pltpu.VMEM((ROWS, WIDTH), BF16),
            pltpu.VMEM((WIDTH, QKV), BF16),
            pltpu.SemaphoreType.DMA((13,)),
        ],
        compiler_params=params(16),
        cost_estimate=cost(2e9, 6e6),
    )(sc, *toks, *w_qkv, cosine, sine)
    low = lax.ppermute(last, "sp", up)
    high = lax.ppermute(first, "sp", down)
    attention = pl.pallas_call(
        attn_kernel,
        out_shape=mixer,
        in_specs=[SMEM, SMEM] + [VMEM] * 4,
        out_specs=VMEM,
        scratch_shapes=[pltpu.VMEM((ROWS + 2 * WINDOW, 256), BF16)],
        compiler_params=params(10),
        cost_estimate=cost(2e9, 2e6),
    )(sc, head_sink_logit, kv, query, low, high)
    conv = pl.pallas_call(
        conv_kernel,
        out_shape=mixer,
        in_specs=[SMEM] + [ANY] * 11 + [VMEM] * 3,
        out_specs=VMEM,
        scratch_shapes=[
            pltpu.VMEM((CONV_ROWS, WIDTH), BF16),
            pltpu.VMEM((WIDTH, CNV), BF16),
            pltpu.VMEM((CONV_ROWS, 256), F32),
            pltpu.SemaphoreType.DMA((13,)),
        ],
        compiler_params=params(18),
        cost_estimate=cost(3e9, 8e6),
    )(sc, *toks, *w_cnv, before, after, conv_taps)
    attn_all = x_ring(attention)
    conv_all = x_ring(conv)
    summed, stats = pl.pallas_call(
        out_kernel,
        out_shape=(
            jax.ShapeDtypeStruct((ROWS, PART), F32),
            jax.ShapeDtypeStruct((2, ROWS), F32),
        ),
        in_specs=[SMEM] + [ANY] * 16,
        out_specs=(VMEM, VMEM),
        scratch_shapes=[
            pltpu.VMEM((ROWS, WIDTH), BF16),
            pltpu.VMEM((PART, WIDTH), BF16),
            pltpu.SemaphoreType.DMA((18,)),
        ],
        compiler_params=params(16),
        cost_estimate=cost(1.6e9, 6e6),
    )(sc, *attn_all, *conv_all, *w_out)
    others = []
    for d in (1, -1, 2):
        others.append(lax.ppermute(stats, "tp", turn(d)))
    return pl.pallas_call(
        norm_kernel,
        out_shape=jax.ShapeDtypeStruct((ROWS, PART), BF16),
        in_specs=[VMEM] * 6,
        out_specs=VMEM,
        compiler_params=params(10),
        cost_estimate=cost(4e6, 3e6),
    )(summed, stats, *others, out_gain.reshape(1, PART))


def solution(mesh):
    return jax.shard_map(
        body,
        mesh=mesh,
        in_specs=(
            P("sp", "tp"),
            P("sp", "tp"),
            P("sp", "tp"),
            P("sp", "tp"),
            P("sp", "tp"),
            P("sp", "tp"),
            P("sp", "tp"),
            P(None, "tp"),
            P("tp"),
            P("tp", "sp"),
            P("tp", "sp"),
            P("tp"),
        ),
        out_specs=P("sp", "tp"),
        check_vma=False,
    )
```

```python
import jax
import jax.numpy as jnp
from jax import lax
from jax.experimental import pallas as pl
from jax.experimental.pallas import tpu as pltpu
from jax.sharding import PartitionSpec as P


HEAD = 128
WINDOW = 128
GRID = 64
NEG_BIG = -1e30
THETA = 10000.0
EPS = 1e-05

ROWS = 768
WIDTH = 2048
PART = 512
QKV = 512
CNV = 768
OUT = 512
ZB = 256


ANY = pl.BlockSpec(memory_space=pl.ANY)
SMEM = pl.BlockSpec(memory_space=pltpu.SMEM)
VMEM = pl.BlockSpec(memory_space=pltpu.VMEM)
F32 = jnp.float32
BF16 = jnp.bfloat16


def chip(z, y, c):
    return ((z % 8) * 4 + y % 4) * 2 + c


def up_down():
    return [
        (chip(z, y, c), chip(z + 1 - 2 * c, y, c))
        for z in range(8)
        for y in range(4)
        for c in range(2)
    ]


def partner():
    return [(i, i ^ 1) for i in range(64)]


def turn(d):
    return [(i, (i + d) % 4) for i in range(4)]


def spread_out_weights():
    pairs = []
    for z in range(8):
        for y in range(4):
            for c in range(2):
                for t in range(4):
                    target = chip((z % 2) * 4 + t, y, c) * 4 + z // 2
                    pairs.append((chip(z, y, c) * 4 + t, target))
    return pairs


def x_ring(block):
    h = block.shape[0] // 2
    r1 = lax.ppermute(block, "tp", turn(1))
    l1 = lax.ppermute(block, "tp", turn(-1))
    r2 = lax.ppermute(r1[:h], "tp", turn(1))
    l2 = lax.ppermute(l1[h:], "tp", turn(-1))
    return [block, r1, l1, r2, l2]


def z_ring(block):
    got = [block]
    for _ in range(1, 5):
        got.append(lax.ppermute(got[-1], "sp", up_down()))
    e = lax.ppermute(jnp.concatenate(got[1:4], 0), "sp", partner())
    return got + [e]


def fetch(copies):
    for c in copies:
        c.start()
    for c in copies:
        c.wait()


def token_copies(sc, toks, tb, sem, top):
    own, r1, l1, r2, l2 = toks
    h = ROWS // 2
    at = [pl.multiple_of(sc[8 + i] * PART, PART) for i in range(4)]
    every = pl.ds(top, ROWS)
    spots = [
        (own, tb.at[every, pl.ds(at[0], PART)]),
        (r1, tb.at[every, pl.ds(at[1], PART)]),
        (l1, tb.at[every, pl.ds(at[2], PART)]),
        (r2, tb.at[pl.ds(top, h), pl.ds(at[3], PART)]),
        (l2, tb.at[pl.ds(top + h, h), pl.ds(at[3], PART)]),
    ]
    return [pltpu.make_async_copy(a, b, sem.at[i]) for i, (a, b) in enumerate(spots)]


def weight_sources(ws):
    block, m1, m2, m3, m4, e = ws
    return [block, m1, m2, m3, m4] + [e.at[pl.ds(k * ZB, ZB), :] for k in range(3)]


def weight_copies(sc, ws, wb, sem, base):
    out = []
    for k, src in enumerate(weight_sources(ws)):
        row = pl.multiple_of(sc[k] * ZB, ZB)
        out.append(pltpu.make_async_copy(src, wb.at[pl.ds(row, ZB), :], sem.at[base + k]))
    return out


def rotate(u, cos, sin, even):
    turned = jnp.where(even, -pltpu.roll(u, 96, 1), pltpu.roll(u, 32, 1))
    return u * cos + turned * sin


def spread_table(ref, first, count):
    by_row = lax.broadcasted_iota(jnp.int32, (GRID, HEAD), 1) < HEAD // 2
    column = ref[16 : 16 + GRID, :]
    groups = [
        jnp.where(by_row, jnp.broadcast_to(ref[g : g + 1, :], (GRID, HEAD)), column)
        for g in range(first, first + count)
    ]
    return jnp.concatenate(groups, 0)


def project_kernel(sc, *refs):
    toks, ws = refs[:5], refs[5:11]
    cos_ref, sin_ref, kv_ref, q_ref, first_ref, last_ref, tb, wb, sem = refs[11:]
    fetch(token_copies(sc, toks, tb, sem, 0) + weight_copies(sc, ws, wb, sem, 5))
    n = 256
    even = (lax.broadcasted_iota(jnp.int32, (n, HEAD), 1) // 32) % 2 == 0
    for i in range(ROWS // n):
        rows = slice(i * n, (i + 1) * n)
        u = jnp.dot(tb[rows, :], wb[...], preferred_element_type=F32)
        cos, sin = (spread_table(t, i * n // GRID, n // GRID) for t in (cos_ref, sin_ref))
        kv_ref[rows, :HEAD] = rotate(u[:, :HEAD], cos, sin, even).astype(BF16)
        kv_ref[rows, HEAD:] = u[:, HEAD : 2 * HEAD].astype(BF16)
        for h in range(2):
            part = u[:, (2 + h) * HEAD : (3 + h) * HEAD]
            q_ref[rows, h * HEAD : (h + 1) * HEAD] = rotate(part, cos, sin, even).astype(BF16)
    first_ref[:WINDOW, :] = kv_ref[:WINDOW, :]
    last_ref[:WINDOW, :] = kv_ref[ROWS - WINDOW :, :]
    for j in range(8):
        rows, lanes = slice(WINDOW + 16 * j, WINDOW + 16 * j + 16), slice(256 * j, 256 * j + 256)
        first_ref[rows, :] = tb[:16, lanes]
        last_ref[rows, :] = tb[ROWS - 16 :, lanes]


def attn_kernel(sc, sink, kv_ref, q_ref, low_ref, high_ref, out_ref, kb):
    kb[:WINDOW, :] = low_ref[:WINDOW, :]
    kb[WINDOW : WINDOW + ROWS, :] = kv_ref[...]
    kb[WINDOW + ROWS :, :] = high_ref[:WINDOW, :]
    place = sc[12]
    two = 2 * WINDOW
    row = lax.broadcasted_iota(jnp.int32, (two, WINDOW), 0) % WINDOW
    col = lax.broadcasted_iota(jnp.int32, (two, WINDOW), 1)
    sinks = jnp.where(
        lax.broadcasted_iota(jnp.int32, (two, 1), 0) < WINDOW, sink[0], sink[1]
    )
    count = ROWS // WINDOW
    for n in range(count):
        left, right = col >= row, col <= row
        if n == 0:
            left = left & (col >= jnp.where(place == 0, WINDOW, 0))
        if n == count - 1:
            right = right & (col < jnp.where(place == 63, 0, WINDOW))
        keys = slice(n * WINDOW, (n + 3) * WINDOW)
        rows = slice(n * WINDOW, (n + 1) * WINDOW)
        k, v = kb[keys, :HEAD], kb[keys, HEAD:]
        q = jnp.concatenate([q_ref[rows, :HEAD], q_ref[rows, HEAD:]], 0)
        s = lax.dot_general(q, k, (((1,), (1,)), ((), ())), preferred_element_type=F32)
        s = s * HEAD ** (-0.5)
        s0 = jnp.where(left, s[:, :WINDOW], NEG_BIG)
        s1 = s[:, WINDOW:two]
        s2 = jnp.where(right, s[:, two:], NEG_BIG)
        top = jnp.maximum(jnp.maximum(s0, s1), s2)
        top = jnp.maximum(jnp.max(top, -1, keepdims=True), sinks)
        w0, w1, w2 = jnp.exp(s0 - top), jnp.exp(s1 - top), jnp.exp(s2 - top)
        total = jnp.sum(w0 + w1 + w2, -1, keepdims=True) + jnp.exp(sinks - top)
        inverse = 1.0 / total
        probs = jnp.concatenate([w0 * inverse, w1 * inverse, w2 * inverse], 1).astype(BF16)
        o = jnp.dot(probs, v, preferred_element_type=F32).astype(BF16)
        out_ref[rows, :HEAD] = o[:WINDOW]
        out_ref[rows, HEAD:] = o[WINDOW:]


CONV_ROWS = ROWS + 32


def conv_kernel(sc, *refs):
    toks, ws = refs[:5], refs[5:11]
    low_ref, high_ref, taps_ref, out_ref, tb, wb, sb, sem = refs[11:]
    copies = token_copies(sc, toks, tb, sem, 16) + weight_copies(sc, ws, wb, sem, 5)
    for c in copies:
        c.start()
    for j in range(8):
        rows, lanes = slice(WINDOW + 16 * j, WINDOW + 16 * j + 16), slice(256 * j, 256 * j + 256)
        tb[:16, lanes] = low_ref[rows, :]
        tb[16 + ROWS :, lanes] = high_ref[rows, :]
    for c in copies:
        c.wait()
    for lo, hi in ((0, 272), (272, 544), (544, 800)):
        both = jnp.dot(tb[lo:hi, :], wb[:, :512], preferred_element_type=F32)
        sb[lo:hi, :] = (both[:, 256:] * both[:, :256]).astype(BF16).astype(F32)
    taps = taps_ref[...].astype(F32)
    for i in range(ROWS // 256):
        r = i * 256
        gate = jnp.dot(tb[16 + r : 272 + r, :], wb[:, 512:], preferred_element_type=F32)
        s = sb[r + 8 : r + 280, :]
        before = pltpu.roll(s, 1, 0)[8:264]
        after = pltpu.roll(s, 271, 0)[8:264]
        conv = before * taps[0:1] + s[8:264] * taps[1:2] + after * taps[2:3]
        out_ref[r : r + 256, :] = (gate * conv).astype(BF16)


SOON = 1792


def mixer_spots(pieces, mb, lane):
    own, r1, l1, r2, l2 = pieces
    h = ROWS // 2
    return [
        (own, mb.at[:, lane : lane + 256]),
        (r1, mb.at[:, lane + 256 : lane + 512]),
        (l1, mb.at[:, lane + 512 : lane + 768]),
        (r2, mb.at[:h, lane + 768 : lane + 1024]),
        (l2, mb.at[h:, lane + 768 : lane + 1024]),
    ]


def out_kernel(sc, *refs):
    attn, conv, ws = refs[:5], refs[5:8], refs[8:14]
    part_ref, tail_ref, mb, wb, sem = refs[14:]
    spots = []
    for k, src in enumerate(weight_sources(ws)):
        row = pl.multiple_of((sc[k] // 4) * ZB, ZB)
        lane = pl.multiple_of(sc[16 + k] * 256, 256)
        spots.append((src.at[:, :256], wb.at[pl.ds(row, ZB), pl.ds(lane, 256)]))
        lane = pl.multiple_of(sc[16 + k] * 256 + 1024, 256)
        spots.append((src.at[:, 256:], wb.at[pl.ds(row, ZB), pl.ds(lane, 256)]))
    spots += mixer_spots(attn, mb, 0) + mixer_spots(conv + (None, None), mb, 1024)[:3]
    fetch([pltpu.make_async_copy(a, b, sem.at[i]) for i, (a, b) in enumerate(spots)])
    for i in range(ROWS // 256):
        rows = slice(i * 256, i * 256 + 256)
        part_ref[rows, :] = lax.dot_general(
            mb[rows, :SOON], wb[:, :SOON], (((1,), (1,)), ((), ())), preferred_element_type=F32
        )
    tail_ref[...] = wb[:, SOON:]


def finish_kernel(part_ref, tail_ref, top_ref, bottom_ref, out_ref, stat_ref):
    h = ROWS // 2
    for i, ref in enumerate((top_ref, bottom_ref)):
        s = part_ref[i * h : i * h + h, :] + lax.dot_general(
            ref[...], tail_ref[...], (((1,), (1,)), ((), ())), preferred_element_type=F32
        )
        out_ref[i * h : i * h + h, :] = s
        mean = jnp.sum(s, -1, keepdims=True) * (1.0 / PART)
        d = s - mean
        second = jnp.sum(d * d, -1, keepdims=True)
        for j in range(h // 128):
            part = slice(j * 128, j * 128 + 128)
            rows = slice(i * h + j * 128, i * h + j * 128 + 128)
            stat_ref[0:1, rows] = jnp.broadcast_to(mean[part], (128, 128)).T[0:1]
            stat_ref[1:2, rows] = jnp.broadcast_to(second[part], (128, 128)).T[0:1]


def norm_kernel(sum_ref, s0, s1, s2, s3, gain_ref, out_ref):
    parts = (s0, s1, s2, s3)
    gain = gain_ref[...]

    def rows_of(i, _):
        r = pl.multiple_of(i * 128, 128)
        rows = pl.ds(r, 128)
        means = [p[0:1, rows] for p in parts]
        mean = (means[0] + means[1] + means[2] + means[3]) * 0.25
        second = sum(p[1:2, rows] for p in parts)
        second = second + PART * sum((m - mean) * (m - mean) for m in means)
        scale = lax.rsqrt(second * (1.0 / WIDTH) + EPS)
        mean = jnp.broadcast_to(mean, (128, 128)).T[:, 0:1]
        scale = jnp.broadcast_to(scale, (128, 128)).T[:, 0:1]
        out_ref[rows, :] = ((sum_ref[rows, :] - mean) * scale * gain).astype(BF16)
        return 0

    lax.fori_loop(0, ROWS // 128, rows_of, 0)


def pack_kernel(*refs):
    out = refs[-1]
    at = 0
    for r in refs[:-1]:
        out[:, at : at + r.shape[1]] = r[...]
        at += r.shape[1]


def cost(flops, read):
    return pl.CostEstimate(flops=int(flops), bytes_accessed=int(read), transcendentals=0)


def params(mib):
    return pltpu.CompilerParams(vmem_limit_bytes=mib * 1024 * 1024)


def rope_tables(first_row):
    half = HEAD // 2
    inverse = THETA ** (-jnp.arange(0, half, 2, dtype=F32) / half)
    count = ROWS // GRID
    row = (first_row + jnp.arange(count, dtype=jnp.int32)).astype(F32)
    column = jnp.arange(GRID, dtype=jnp.int32).astype(F32)
    place = jnp.concatenate([row, jnp.zeros((4,), F32), column])
    angles = place[:, None] * jnp.concatenate([inverse] * 4)
    return jnp.cos(angles), jnp.sin(angles)


def body(
    tokens,
    query_weight,
    key_projection,
    value_projection,
    conv_in_weight,
    conv_gate_out,
    conv_gate_in,
    conv_taps,
    head_sink_logit,
    out_attn_weight,
    out_conv_weight,
    out_gain,
):
    s = lax.axis_index("sp")
    x = lax.axis_index("tp")
    z, core = s // 8, s % 2
    sign = 2 * core - 1
    steps = jnp.array([0, 1, 2, 3, 4, -1, -2, -3], jnp.int32)
    turns = jnp.array([0, -1, 1, 2], jnp.int32)
    plane_of = (z + sign * steps + 8) % 8
    apart = (plane_of - x) % 4
    slot = jnp.where(apart == 3, 1, jnp.where(apart == 0, 0, apart + 1))
    sc = jnp.concatenate(
        [plane_of, (x + turns + 4) % 4, jnp.full((4,), s, jnp.int32), slot]
    ).astype(jnp.int32)

    toks = x_ring(tokens)
    up = [(i, i + 1) for i in range(63)]
    down = [(i + 1, i) for i in range(63)]
    stacked = jnp.concatenate([out_attn_weight.T, out_conv_weight.T], 1)
    stacked = lax.ppermute(stacked, ("sp", "tp"), spread_out_weights())

    packed = pl.pallas_call(
        pack_kernel,
        out_shape=jax.ShapeDtypeStruct((32, QKV + CNV + OUT), BF16),
        in_specs=[VMEM] * 7,
        out_specs=VMEM,
        cost_estimate=cost(1e6, 3e5),
    )(
        key_projection,
        value_projection,
        query_weight,
        conv_in_weight,
        conv_gate_in,
        conv_gate_out,
        stacked,
    )
    planes = [[chip(z, y, c) for y in range(4) for c in range(2)] for z in range(8)]
    plane = lax.all_gather(packed, "sp", axis=0, tiled=True, axis_index_groups=planes)
    w_qkv = z_ring(plane[:, :QKV])
    w_cnv = z_ring(plane[:, QKV : QKV + CNV])
    w_out = z_ring(plane[:, QKV + CNV :])

    cosine, sine = rope_tables(s * (ROWS // GRID))

    edge = jax.ShapeDtypeStruct((2 * WINDOW, 256), BF16)
    mixer = jax.ShapeDtypeStruct((ROWS, 256), BF16)
    kv, query, first, last = pl.pallas_call(
        project_kernel,
        out_shape=(mixer, mixer, edge, edge),
        in_specs=[SMEM] + [ANY] * 11 + [VMEM] * 2,
        out_specs=(VMEM,) * 4,
        scratch_shapes=[
            pltpu.VMEM((ROWS, WIDTH), BF16),
            pltpu.VMEM((WIDTH, QKV), BF16),
            pltpu.SemaphoreType.DMA((13,)),
        ],
        compiler_params=params(16),
        cost_estimate=cost(2e9, 6e6),
    )(sc, *toks, *w_qkv, cosine, sine)
    low = lax.ppermute(last, "sp", up)
    high = lax.ppermute(first, "sp", down)
    attention = pl.pallas_call(
        attn_kernel,
        out_shape=mixer,
        in_specs=[SMEM, SMEM] + [VMEM] * 4,
        out_specs=VMEM,
        scratch_shapes=[pltpu.VMEM((ROWS + 2 * WINDOW, 256), BF16)],
        compiler_params=params(10),
        cost_estimate=cost(2e9, 2e6),
    )(sc, head_sink_logit, kv, query, low, high)
    conv = pl.pallas_call(
        conv_kernel,
        out_shape=mixer,
        in_specs=[SMEM] + [ANY] * 11 + [VMEM] * 3,
        out_specs=VMEM,
        scratch_shapes=[
            pltpu.VMEM((CONV_ROWS, WIDTH), BF16),
            pltpu.VMEM((WIDTH, CNV), BF16),
            pltpu.VMEM((CONV_ROWS, 256), F32),
            pltpu.SemaphoreType.DMA((13,)),
        ],
        compiler_params=params(18),
        cost_estimate=cost(3e9, 8e6),
    )(sc, *toks, *w_cnv, low, high, conv_taps)
    attn_all = x_ring(attention)
    conv_all = x_ring(conv)
    partial, tail = pl.pallas_call(
        out_kernel,
        out_shape=(
            jax.ShapeDtypeStruct((ROWS, PART), F32),
            jax.ShapeDtypeStruct((PART, WIDTH - SOON), BF16),
        ),
        in_specs=[SMEM] + [ANY] * 14,
        out_specs=(VMEM, VMEM),
        scratch_shapes=[
            pltpu.VMEM((ROWS, WIDTH), BF16),
            pltpu.VMEM((PART, WIDTH), BF16),
            pltpu.SemaphoreType.DMA((24,)),
        ],
        compiler_params=params(16),
        cost_estimate=cost(1.4e9, 6e6),
    )(sc, *attn_all, *conv_all[:3], *w_out)
    summed, stats = pl.pallas_call(
        finish_kernel,
        out_shape=(
            jax.ShapeDtypeStruct((ROWS, PART), F32),
            jax.ShapeDtypeStruct((2, ROWS), F32),
        ),
        in_specs=[VMEM] * 4,
        out_specs=(VMEM, VMEM),
        compiler_params=params(14),
        cost_estimate=cost(4e8, 4e6),
    )(partial, tail, *conv_all[3:])
    others = []
    for d in (1, -1, 2):
        others.append(lax.ppermute(stats, "tp", turn(d)))
    return pl.pallas_call(
        norm_kernel,
        out_shape=jax.ShapeDtypeStruct((ROWS, PART), BF16),
        in_specs=[VMEM] * 6,
        out_specs=VMEM,
        compiler_params=params(10),
        cost_estimate=cost(4e6, 3e6),
    )(summed, stats, *others, out_gain.reshape(1, PART))


def solution(mesh):
    return jax.shard_map(
        body,
        mesh=mesh,
        in_specs=(
            P("sp", "tp"),
            P("sp", "tp"),
            P("sp", "tp"),
            P("sp", "tp"),
            P("sp", "tp"),
            P("sp", "tp"),
            P("sp", "tp"),
            P(None, "tp"),
            P("tp"),
            P("tp", "sp"),
            P("tp", "sp"),
            P("tp"),
        ),
        out_specs=P("sp", "tp"),
        check_vma=False,
    )
```

```python
import jax
import jax.numpy as jnp
from jax import lax
from jax.experimental import pallas as pl
from jax.experimental.pallas import tpu as pltpu
from jax.sharding import PartitionSpec as P


HEAD = 128
WINDOW = 128
GRID = 64
NEG_BIG = -1e30
THETA = 10000.0
EPS = 1e-05

ROWS = 768
WIDTH = 2048
PART = 512
QKV = 512
CNV = 768
OUT = 512
ZB = 256


ANY = pl.BlockSpec(memory_space=pl.ANY)
SMEM = pl.BlockSpec(memory_space=pltpu.SMEM)
VMEM = pl.BlockSpec(memory_space=pltpu.VMEM)
F32 = jnp.float32
BF16 = jnp.bfloat16


def chip(z, y, c):
    return ((z % 8) * 4 + y % 4) * 2 + c


def up_down():
    return [
        (chip(z, y, c), chip(z + 1 - 2 * c, y, c))
        for z in range(8)
        for y in range(4)
        for c in range(2)
    ]


def partner():
    return [(i, i ^ 1) for i in range(64)]


def turn(d):
    return [(i, (i + d) % 4) for i in range(4)]


def spread_out_weights():
    pairs = []
    for z in range(8):
        for y in range(4):
            for c in range(2):
                for t in range(4):
                    target = chip((z % 2) * 4 + t, y, c) * 4 + z // 2
                    pairs.append((chip(z, y, c) * 4 + t, target))
    return pairs


def x_ring(block):
    h = block.shape[0] // 2
    r1 = lax.ppermute(block, "tp", turn(1))
    l1 = lax.ppermute(block, "tp", turn(-1))
    r2 = lax.ppermute(r1[:h], "tp", turn(1))
    l2 = lax.ppermute(l1[h:], "tp", turn(-1))
    return [block, r1, l1, r2, l2]


def z_ring(block):
    got = [block]
    for _ in range(1, 5):
        got.append(lax.ppermute(got[-1], "sp", up_down()))
    e = lax.ppermute(jnp.concatenate(got[1:4], 0), "sp", partner())
    return got + [e]


def start(copies):
    for c in copies:
        c.start()


def wait(copies):
    for c in copies:
        c.wait()


def token_copies(sc, toks, tb, sem, top):
    own, r1, l1, r2, l2 = toks
    h = ROWS // 2
    at = [pl.multiple_of(sc[8 + i] * PART, PART) for i in range(4)]
    halves = []
    for j, last in enumerate((r2, l2)):
        rows, spots = pl.ds(j * h, h), pl.ds(top + j * h, h)
        sources = [own.at[rows, :], r1.at[rows, :], l1.at[rows, :], last]
        halves.append(
            [
                pltpu.make_async_copy(
                    src, tb.at[spots, pl.ds(at[i], PART)], sem.at[8 + 4 * j + i]
                )
                for i, src in enumerate(sources)
            ]
        )
    return halves


def weight_sources(ws):
    block, m1, m2, m3, m4, e = ws
    return [block, m1, m2, m3, m4] + [e.at[pl.ds(k * ZB, ZB), :] for k in range(3)]


def weight_copies(sc, ws, wb, sem):
    out = []
    for k, src in enumerate(weight_sources(ws)):
        row = pl.multiple_of(sc[k] * ZB, ZB)
        out.append(pltpu.make_async_copy(src, wb.at[pl.ds(row, ZB), :], sem.at[k]))
    return out


def rotate(u, cos, sin, even):
    turned = jnp.where(even, -pltpu.roll(u, 96, 1), pltpu.roll(u, 32, 1))
    return u * cos + turned * sin


def spread_table(ref, first, count):
    by_row = lax.broadcasted_iota(jnp.int32, (GRID, HEAD), 1) < HEAD // 2
    column = ref[16 : 16 + GRID, :]
    groups = [
        jnp.where(by_row, jnp.broadcast_to(ref[g : g + 1, :], (GRID, HEAD)), column)
        for g in range(first, first + count)
    ]
    return jnp.concatenate(groups, 0)


def project_kernel(sc, *refs):
    toks, ws = refs[:5], refs[5:11]
    cos_ref, sin_ref, kv_ref, q_ref, first_ref, last_ref, tb, wb, sem = refs[11:]
    halves = token_copies(sc, toks, tb, sem, 0)
    weights = weight_copies(sc, ws, wb, sem)
    start(weights + halves[0] + halves[1])
    wait(weights + halves[0])
    n = ROWS // 4
    even = (lax.broadcasted_iota(jnp.int32, (n, HEAD), 1) // 32) % 2 == 0
    for i in range(ROWS // n):
        if i == 2:
            wait(halves[1])
        rows = slice(i * n, (i + 1) * n)
        u = jnp.dot(tb[rows, :], wb[...], preferred_element_type=F32)
        cos, sin = (spread_table(t, i * n // GRID, n // GRID) for t in (cos_ref, sin_ref))
        kv_ref[rows, :HEAD] = rotate(u[:, :HEAD], cos, sin, even).astype(BF16)
        kv_ref[rows, HEAD:] = u[:, HEAD : 2 * HEAD].astype(BF16)
        for h in range(2):
            part = u[:, (2 + h) * HEAD : (3 + h) * HEAD]
            q_ref[rows, h * HEAD : (h + 1) * HEAD] = rotate(part, cos, sin, even).astype(BF16)
    first_ref[:WINDOW, :] = kv_ref[:WINDOW, :]
    last_ref[:WINDOW, :] = kv_ref[ROWS - WINDOW :, :]
    for j in range(8):
        rows, lanes = slice(WINDOW + 16 * j, WINDOW + 16 * j + 16), slice(256 * j, 256 * j + 256)
        first_ref[rows, :] = tb[:16, lanes]
        last_ref[rows, :] = tb[ROWS - 16 :, lanes]


def attn_kernel(sc, sink, kv_ref, q_ref, low_ref, high_ref, out_ref, kb):
    kb[:WINDOW, :] = low_ref[:WINDOW, :]
    kb[WINDOW : WINDOW + ROWS, :] = kv_ref[...]
    kb[WINDOW + ROWS :, :] = high_ref[:WINDOW, :]
    place = sc[12]
    two = 2 * WINDOW
    row = lax.broadcasted_iota(jnp.int32, (two, WINDOW), 0) % WINDOW
    col = lax.broadcasted_iota(jnp.int32, (two, WINDOW), 1)
    sinks = jnp.where(
        lax.broadcasted_iota(jnp.int32, (two, 1), 0) < WINDOW, sink[0], sink[1]
    )
    count = ROWS // WINDOW
    for n in range(count):
        left, right = col >= row, col <= row
        if n == 0:
            left = left & (col >= jnp.where(place == 0, WINDOW, 0))
        if n == count - 1:
            right = right & (col < jnp.where(place == 63, 0, WINDOW))
        keys = slice(n * WINDOW, (n + 3) * WINDOW)
        rows = slice(n * WINDOW, (n + 1) * WINDOW)
        k, v = kb[keys, :HEAD], kb[keys, HEAD:]
        q = jnp.concatenate([q_ref[rows, :HEAD], q_ref[rows, HEAD:]], 0)
        s = lax.dot_general(q, k, (((1,), (1,)), ((), ())), preferred_element_type=F32)
        s = s * HEAD ** (-0.5)
        s0 = jnp.where(left, s[:, :WINDOW], NEG_BIG)
        s1 = s[:, WINDOW:two]
        s2 = jnp.where(right, s[:, two:], NEG_BIG)
        top = jnp.maximum(jnp.maximum(s0, s1), s2)
        top = jnp.maximum(jnp.max(top, -1, keepdims=True), sinks)
        w0, w1, w2 = jnp.exp(s0 - top), jnp.exp(s1 - top), jnp.exp(s2 - top)
        total = jnp.sum(w0 + w1 + w2, -1, keepdims=True) + jnp.exp(sinks - top)
        inverse = 1.0 / total
        probs = jnp.concatenate([w0 * inverse, w1 * inverse, w2 * inverse], 1).astype(BF16)
        o = jnp.dot(probs, v, preferred_element_type=F32).astype(BF16)
        out_ref[rows, :HEAD] = o[:WINDOW]
        out_ref[rows, HEAD:] = o[WINDOW:]


CONV_ROWS = ROWS + 32


def conv_kernel(sc, *refs):
    toks, ws = refs[:5], refs[5:11]
    low_ref, high_ref, taps_ref, out_ref, tb, wb, sb, sem = refs[11:]
    halves = token_copies(sc, toks, tb, sem, 16)
    weights = weight_copies(sc, ws, wb, sem)
    start(weights + halves[0] + halves[1])
    for j in range(8):
        rows, lanes = slice(WINDOW + 16 * j, WINDOW + 16 * j + 16), slice(256 * j, 256 * j + 256)
        tb[:16, lanes] = low_ref[rows, :]
        tb[16 + ROWS :, lanes] = high_ref[rows, :]
    wait(weights + halves[0])
    for lo, hi in ((0, 208), (208, 400), (400, 592), (592, 800)):
        if lo == 400:
            wait(halves[1])
        both = jnp.dot(tb[lo:hi, :], wb[:, :512], preferred_element_type=F32)
        sb[lo:hi, :] = (both[:, 256:] * both[:, :256]).astype(BF16).astype(F32)
    taps = taps_ref[...].astype(F32)
    for i in range(ROWS // 256):
        r = i * 256
        gate = jnp.dot(tb[16 + r : 272 + r, :], wb[:, 512:], preferred_element_type=F32)
        s = sb[r + 8 : r + 280, :]
        before = pltpu.roll(s, 1, 0)[8:264]
        after = pltpu.roll(s, 271, 0)[8:264]
        conv = before * taps[0:1] + s[8:264] * taps[1:2] + after * taps[2:3]
        out_ref[r : r + 256, :] = (gate * conv).astype(BF16)


SOON = 1792


def mixer_spots(pieces, mb, lane):
    own, r1, l1, r2, l2 = pieces
    h = ROWS // 2
    return [
        (own, mb.at[:, lane : lane + 256]),
        (r1, mb.at[:, lane + 256 : lane + 512]),
        (l1, mb.at[:, lane + 512 : lane + 768]),
        (r2, mb.at[:h, lane + 768 : lane + 1024]),
        (l2, mb.at[h:, lane + 768 : lane + 1024]),
    ]


def out_kernel(sc, *refs):
    attn, conv, ws = refs[:5], refs[5:8], refs[8:14]
    part_ref, tail_ref, mb, wb, sem = refs[14:]
    spots = []
    for k, src in enumerate(weight_sources(ws)):
        row = pl.multiple_of((sc[k] // 4) * ZB, ZB)
        lane = pl.multiple_of(sc[16 + k] * 256, 256)
        spots.append((src.at[:, :256], wb.at[pl.ds(row, ZB), pl.ds(lane, 256)]))
        lane = pl.multiple_of(sc[16 + k] * 256 + 1024, 256)
        spots.append((src.at[:, 256:], wb.at[pl.ds(row, ZB), pl.ds(lane, 256)]))
    spots += mixer_spots(attn, mb, 0) + mixer_spots(conv + (None, None), mb, 1024)[:3]
    copies = [pltpu.make_async_copy(a, b, sem.at[i]) for i, (a, b) in enumerate(spots)]
    start(copies)
    wait(copies)
    for i in range(ROWS // 256):
        rows = slice(i * 256, i * 256 + 256)
        part_ref[rows, :] = lax.dot_general(
            mb[rows, :SOON], wb[:, :SOON], (((1,), (1,)), ((), ())), preferred_element_type=F32
        )
    tail_ref[...] = wb[:, SOON:]


def finish_kernel(part_ref, tail_ref, top_ref, bottom_ref, out_ref, stat_ref):
    h = ROWS // 2
    for i, ref in enumerate((top_ref, bottom_ref)):
        s = part_ref[i * h : i * h + h, :] + lax.dot_general(
            ref[...], tail_ref[...], (((1,), (1,)), ((), ())), preferred_element_type=F32
        )
        out_ref[i * h : i * h + h, :] = s
        mean = jnp.sum(s, -1, keepdims=True) * (1.0 / PART)
        d = s - mean
        second = jnp.sum(d * d, -1, keepdims=True)
        for j in range(h // 128):
            part = slice(j * 128, j * 128 + 128)
            rows = slice(i * h + j * 128, i * h + j * 128 + 128)
            stat_ref[0:1, rows] = jnp.broadcast_to(mean[part], (128, 128)).T[0:1]
            stat_ref[1:2, rows] = jnp.broadcast_to(second[part], (128, 128)).T[0:1]


def norm_kernel(sum_ref, s0, s1, s2, s3, gain_ref, out_ref, buf, sem):
    parts = (s0, s1, s2, s3)
    gain = gain_ref[...]

    copies = []
    for i in range(ROWS // 128):
        rows = slice(i * 128, i * 128 + 128)
        means = [p[0:1, rows] for p in parts]
        mean = (means[0] + means[1] + means[2] + means[3]) * 0.25
        second = sum(p[1:2, rows] for p in parts)
        second = second + PART * sum((m - mean) * (m - mean) for m in means)
        scale = lax.rsqrt(second * (1.0 / WIDTH) + EPS)
        mean = jnp.broadcast_to(mean, (128, 128)).T[:, 0:1]
        scale = jnp.broadcast_to(scale, (128, 128)).T[:, 0:1]
        buf[rows, :] = ((sum_ref[rows, :] - mean) * scale * gain).astype(BF16)
        copies.append(pltpu.make_async_copy(buf.at[rows, :], out_ref.at[rows, :], sem.at[i]))
        copies[-1].start()
    wait(copies)


def pack_kernel(*refs):
    out = refs[-1]
    at = 0
    for r in refs[:-1]:
        out[:, at : at + r.shape[1]] = r[...]
        at += r.shape[1]


def cost(flops, read):
    return pl.CostEstimate(flops=int(flops), bytes_accessed=int(read), transcendentals=0)


def params(mib):
    return pltpu.CompilerParams(vmem_limit_bytes=mib * 1024 * 1024)


def rope_tables(first_row):
    half = HEAD // 2
    inverse = THETA ** (-jnp.arange(0, half, 2, dtype=F32) / half)
    count = ROWS // GRID
    row = (first_row + jnp.arange(count, dtype=jnp.int32)).astype(F32)
    column = jnp.arange(GRID, dtype=jnp.int32).astype(F32)
    place = jnp.concatenate([row, jnp.zeros((4,), F32), column])
    angles = place[:, None] * jnp.concatenate([inverse] * 4)
    return jnp.cos(angles), jnp.sin(angles)


def body(
    tokens,
    query_weight,
    key_projection,
    value_projection,
    conv_in_weight,
    conv_gate_out,
    conv_gate_in,
    conv_taps,
    head_sink_logit,
    out_attn_weight,
    out_conv_weight,
    out_gain,
):
    s = lax.axis_index("sp")
    x = lax.axis_index("tp")
    z, core = s // 8, s % 2
    sign = 2 * core - 1
    steps = jnp.array([0, 1, 2, 3, 4, -1, -2, -3], jnp.int32)
    turns = jnp.array([0, -1, 1, 2], jnp.int32)
    plane_of = (z + sign * steps + 8) % 8
    apart = (plane_of - x) % 4
    slot = jnp.where(apart == 3, 1, jnp.where(apart == 0, 0, apart + 1))
    sc = jnp.concatenate(
        [plane_of, (x + turns + 4) % 4, jnp.full((4,), s, jnp.int32), slot]
    ).astype(jnp.int32)

    toks = x_ring(tokens)
    up = [(i, i + 1) for i in range(63)]
    down = [(i + 1, i) for i in range(63)]
    stacked = jnp.concatenate([out_attn_weight.T, out_conv_weight.T], 1)
    stacked = lax.ppermute(stacked, ("sp", "tp"), spread_out_weights())

    packed = pl.pallas_call(
        pack_kernel,
        out_shape=jax.ShapeDtypeStruct((32, QKV + CNV + OUT), BF16),
        in_specs=[VMEM] * 7,
        out_specs=VMEM,
        cost_estimate=cost(1e6, 3e5),
    )(
        key_projection,
        value_projection,
        query_weight,
        conv_in_weight,
        conv_gate_in,
        conv_gate_out,
        stacked,
    )
    planes = [[chip(z, y, c) for y in range(4) for c in range(2)] for z in range(8)]
    plane = lax.all_gather(packed, "sp", axis=0, tiled=True, axis_index_groups=planes)
    w_qkv = z_ring(plane[:, :QKV])
    w_cnv = z_ring(plane[:, QKV : QKV + CNV])
    w_out = z_ring(plane[:, QKV + CNV :])

    cosine, sine = rope_tables(s * (ROWS // GRID))

    edge = jax.ShapeDtypeStruct((2 * WINDOW, 256), BF16)
    mixer = jax.ShapeDtypeStruct((ROWS, 256), BF16)
    kv, query, first, last = pl.pallas_call(
        project_kernel,
        out_shape=(mixer, mixer, edge, edge),
        in_specs=[SMEM] + [ANY] * 11 + [VMEM] * 2,
        out_specs=(VMEM,) * 4,
        scratch_shapes=[
            pltpu.VMEM((ROWS, WIDTH), BF16),
            pltpu.VMEM((WIDTH, QKV), BF16),
            pltpu.SemaphoreType.DMA((16,)),
        ],
        compiler_params=params(16),
        cost_estimate=cost(2e9, 6e6),
    )(sc, *toks, *w_qkv, cosine, sine)
    low = lax.ppermute(last, "sp", up)
    high = lax.ppermute(first, "sp", down)
    attention = pl.pallas_call(
        attn_kernel,
        out_shape=mixer,
        in_specs=[SMEM, SMEM] + [VMEM] * 4,
        out_specs=VMEM,
        scratch_shapes=[pltpu.VMEM((ROWS + 2 * WINDOW, 256), BF16)],
        compiler_params=params(10),
        cost_estimate=cost(2e9, 2e6),
    )(sc, head_sink_logit, kv, query, low, high)
    conv = pl.pallas_call(
        conv_kernel,
        out_shape=mixer,
        in_specs=[SMEM] + [ANY] * 11 + [VMEM] * 3,
        out_specs=VMEM,
        scratch_shapes=[
            pltpu.VMEM((CONV_ROWS, WIDTH), BF16),
            pltpu.VMEM((WIDTH, CNV), BF16),
            pltpu.VMEM((CONV_ROWS, 256), F32),
            pltpu.SemaphoreType.DMA((16,)),
        ],
        compiler_params=params(18),
        cost_estimate=cost(3e9, 8e6),
    )(sc, *toks, *w_cnv, low, high, conv_taps)
    attn_all = x_ring(attention)
    conv_all = x_ring(conv)
    partial, tail = pl.pallas_call(
        out_kernel,
        out_shape=(
            jax.ShapeDtypeStruct((ROWS, PART), F32),
            jax.ShapeDtypeStruct((PART, WIDTH - SOON), BF16),
        ),
        in_specs=[SMEM] + [ANY] * 14,
        out_specs=(VMEM, VMEM),
        scratch_shapes=[
            pltpu.VMEM((ROWS, WIDTH), BF16),
            pltpu.VMEM((PART, WIDTH), BF16),
            pltpu.SemaphoreType.DMA((24,)),
        ],
        compiler_params=params(16),
        cost_estimate=cost(1.4e9, 6e6),
    )(sc, *attn_all, *conv_all[:3], *w_out)
    summed, stats = pl.pallas_call(
        finish_kernel,
        out_shape=(
            jax.ShapeDtypeStruct((ROWS, PART), F32),
            jax.ShapeDtypeStruct((2, ROWS), F32),
        ),
        in_specs=[VMEM] * 4,
        out_specs=(VMEM, VMEM),
        compiler_params=params(14),
        cost_estimate=cost(4e8, 4e6),
    )(partial, tail, *conv_all[3:])
    others = []
    for d in (1, -1, 2):
        others.append(lax.ppermute(stats, "tp", turn(d)))
    return pl.pallas_call(
        norm_kernel,
        out_shape=jax.ShapeDtypeStruct((ROWS, PART), BF16),
        in_specs=[VMEM] * 6,
        out_specs=ANY,
        scratch_shapes=[
            pltpu.VMEM((ROWS, PART), BF16),
            pltpu.SemaphoreType.DMA((ROWS // 128,)),
        ],
        compiler_params=params(10),
        cost_estimate=cost(4e6, 3e6),
    )(summed, stats, *others, out_gain.reshape(1, PART))


def solution(mesh):
    return jax.shard_map(
        body,
        mesh=mesh,
        in_specs=(
            P("sp", "tp"),
            P("sp", "tp"),
            P("sp", "tp"),
            P("sp", "tp"),
            P("sp", "tp"),
            P("sp", "tp"),
            P("sp", "tp"),
            P(None, "tp"),
            P("tp"),
            P("tp", "sp"),
            P("tp", "sp"),
            P("tp"),
        ),
        out_specs=P("sp", "tp"),
        check_vma=False,
    )
```

```python
import jax
import jax.numpy as jnp
from jax import lax
from jax.experimental import pallas as pl
from jax.experimental.pallas import tpu as pltpu
from jax.sharding import PartitionSpec as P


HEAD = 128
WINDOW = 128
GRID = 64
NEG_BIG = -1e30
THETA = 10000.0
EPS = 1e-05

ROWS = 768
WIDTH = 2048
PART = 512
QKV = 512
CNV = 768
OUT = 512
ZB = 256


ANY = pl.BlockSpec(memory_space=pl.ANY)
SMEM = pl.BlockSpec(memory_space=pltpu.SMEM)
VMEM = pl.BlockSpec(memory_space=pltpu.VMEM)
F32 = jnp.float32
BF16 = jnp.bfloat16


def chip(z, y, c):
    return ((z % 8) * 4 + y % 4) * 2 + c


def up_down():
    return [
        (chip(z, y, c), chip(z + 1 - 2 * c, y, c))
        for z in range(8)
        for y in range(4)
        for c in range(2)
    ]


def partner():
    return [(i, i ^ 1) for i in range(64)]


def turn(d):
    return [(i, (i + d) % 4) for i in range(4)]


def spread_out_weights():
    pairs = []
    for z in range(8):
        for y in range(4):
            for c in range(2):
                for t in range(4):
                    target = chip((z % 2) * 4 + t, y, c) * 4 + z // 2
                    pairs.append((chip(z, y, c) * 4 + t, target))
    return pairs


def x_ring(block):
    h = block.shape[0] // 2
    r1 = lax.ppermute(block, "tp", turn(1))
    l1 = lax.ppermute(block, "tp", turn(-1))
    r2 = lax.ppermute(r1[:h], "tp", turn(1))
    l2 = lax.ppermute(l1[h:], "tp", turn(-1))
    return [block, r1, l1, r2, l2]


def x_pass(block, way):
    r1 = lax.ppermute(block, "tp", turn(1))
    l1 = lax.ppermute(block, "tp", turn(-1))
    far = lax.ppermute(r1 if way == 1 else l1, "tp", turn(way))
    return [block, r1, l1, far]


def z_ring(block):
    got = [block]
    for _ in range(1, 5):
        got.append(lax.ppermute(got[-1], "sp", up_down()))
    e = lax.ppermute(jnp.concatenate(got[1:4], 0), "sp", partner())
    return got + [e]


def start(copies):
    for c in copies:
        c.start()


def wait(copies):
    for c in copies:
        c.wait()


def token_copies(sc, toks, halos, tb, sem, reach):
    h = ROWS // 2
    groups = ([], [])
    for i in range(4):
        lanes = pl.ds(pl.multiple_of(sc[8 + i] * PART, PART), PART)
        low = halos[i].at[WINDOW - reach : WINDOW, :]
        high = halos[i].at[WINDOW : WINDOW + reach, :]
        spots = (
            (0, low, 0, reach),
            (0, toks[i].at[:h, :], reach, h),
            (1, toks[i].at[h:, :], reach + h, h),
            (1, high, reach + ROWS, reach),
        )
        for j, (group, src, row, count) in enumerate(spots):
            dst = tb.at[pl.ds(row, count), lanes]
            groups[group].append(pltpu.make_async_copy(src, dst, sem.at[8 + 4 * i + j]))
    return groups


def weight_sources(ws):
    block, m1, m2, m3, m4, e = ws
    return [block, m1, m2, m3, m4] + [e.at[pl.ds(k * ZB, ZB), :] for k in range(3)]


def weight_copies(sc, ws, wb, sem):
    out = []
    for k, src in enumerate(weight_sources(ws)):
        row = pl.multiple_of(sc[k] * ZB, ZB)
        out.append(pltpu.make_async_copy(src, wb.at[pl.ds(row, ZB), :], sem.at[k]))
    return out


def rotate(u, cos, sin, even):
    turned = jnp.where(even, -pltpu.roll(u, 96, 1), pltpu.roll(u, 32, 1))
    return u * cos + turned * sin


def spread_table(ref, first, count):
    by_row = lax.broadcasted_iota(jnp.int32, (GRID, HEAD), 1) < HEAD // 2
    column = ref[16 : 16 + GRID, :]
    groups = [
        jnp.where(by_row, jnp.broadcast_to(ref[g : g + 1, :], (GRID, HEAD)), column)
        for g in range(first, first + count)
    ]
    return jnp.concatenate(groups, 0)


EXT = ROWS + 2 * WINDOW


def project_kernel(sc, *refs):
    toks, halos, ws = refs[:4], refs[4:8], refs[8:14]
    cos_ref, sin_ref, kv_ref, q_ref, tb, wb, sem = refs[14:]
    halves = token_copies(sc, toks, halos, tb, sem, WINDOW)
    weights = weight_copies(sc, ws, wb, sem)
    start(weights + halves[0] + halves[1])
    wait(weights + halves[0])
    n = 256
    even = (lax.broadcasted_iota(jnp.int32, (n, HEAD), 1) // 32) % 2 == 0

    def keys(i):
        rows = slice(i * n, i * n + n)
        u = jnp.dot(tb[rows, :], wb[:, :256], preferred_element_type=F32)
        cos, sin = (spread_table(t, i * n // GRID, n // GRID) for t in (cos_ref, sin_ref))
        kv_ref[rows, :HEAD] = rotate(u[:, :HEAD], cos, sin, even).astype(BF16)
        kv_ref[rows, HEAD:] = u[:, HEAD:].astype(BF16)

    def queries(i):
        first = i * n + WINDOW
        u = jnp.dot(tb[first : first + n, :], wb[:, 256:], preferred_element_type=F32)
        cos, sin = (spread_table(t, first // GRID, n // GRID) for t in (cos_ref, sin_ref))
        for h in range(2):
            lanes = slice(h * HEAD, (h + 1) * HEAD)
            q_ref[i * n : i * n + n, lanes] = rotate(u[:, lanes], cos, sin, even).astype(BF16)

    keys(0)
    keys(1)
    queries(0)
    wait(halves[1])
    keys(2)
    keys(3)
    queries(1)
    queries(2)


def attn_kernel(sc, sink, kb, q_ref, out_ref):
    place = sc[12]
    two = 2 * WINDOW
    row = lax.broadcasted_iota(jnp.int32, (two, WINDOW), 0) % WINDOW
    col = lax.broadcasted_iota(jnp.int32, (two, WINDOW), 1)
    sinks = jnp.where(
        lax.broadcasted_iota(jnp.int32, (two, 1), 0) < WINDOW, sink[0], sink[1]
    )
    count = ROWS // WINDOW
    for n in range(count):
        left, right = col >= row, col <= row
        if n == 0:
            left = left & (col >= jnp.where(place == 0, WINDOW, 0))
        if n == count - 1:
            right = right & (col < jnp.where(place == 63, 0, WINDOW))
        keys = slice(n * WINDOW, (n + 3) * WINDOW)
        rows = slice(n * WINDOW, (n + 1) * WINDOW)
        k, v = kb[keys, :HEAD], kb[keys, HEAD:]
        q = jnp.concatenate([q_ref[rows, :HEAD], q_ref[rows, HEAD:]], 0)
        s = lax.dot_general(q, k, (((1,), (1,)), ((), ())), preferred_element_type=F32)
        s = s * HEAD ** (-0.5)
        s0 = jnp.where(left, s[:, :WINDOW], NEG_BIG)
        s1 = s[:, WINDOW:two]
        s2 = jnp.where(right, s[:, two:], NEG_BIG)
        top = jnp.maximum(jnp.maximum(s0, s1), s2)
        top = jnp.maximum(jnp.max(top, -1, keepdims=True), sinks)
        w0, w1, w2 = jnp.exp(s0 - top), jnp.exp(s1 - top), jnp.exp(s2 - top)
        total = jnp.sum(w0 + w1 + w2, -1, keepdims=True) + jnp.exp(sinks - top)
        inverse = 1.0 / total
        probs = jnp.concatenate([w0 * inverse, w1 * inverse, w2 * inverse], 1).astype(BF16)
        o = jnp.dot(probs, v, preferred_element_type=F32).astype(BF16)
        out_ref[rows, :HEAD] = o[:WINDOW]
        out_ref[rows, HEAD:] = o[WINDOW:]


CONV_ROWS = ROWS + 32


def conv_kernel(sc, *refs):
    toks, halos, ws = refs[:4], refs[4:8], refs[8:14]
    taps_ref, out_ref, tb, wb, sb, sem = refs[14:]
    halves = token_copies(sc, toks, halos, tb, sem, 16)
    weights = weight_copies(sc, ws, wb, sem)
    start(weights + halves[0] + halves[1])
    wait(weights + halves[0])
    for lo, hi in ((0, 272), (272, 544), (544, 800)):
        if lo == 272:
            wait(halves[1])
        both = jnp.dot(tb[lo:hi, :], wb[:, :512], preferred_element_type=F32)
        sb[lo:hi, :] = (both[:, 256:] * both[:, :256]).astype(BF16).astype(F32)
    taps = taps_ref[...].astype(F32)
    for i in range(ROWS // 256):
        r = i * 256
        gate = jnp.dot(tb[16 + r : 272 + r, :], wb[:, 512:], preferred_element_type=F32)
        s = sb[r + 8 : r + 280, :]
        before = pltpu.roll(s, 1, 0)[8:264]
        after = pltpu.roll(s, 271, 0)[8:264]
        conv = before * taps[0:1] + s[8:264] * taps[1:2] + after * taps[2:3]
        out_ref[r : r + 256, :] = (gate * conv).astype(BF16)


SOON = 1792


def mixer_spots(pieces, mb, lane):
    own, r1, l1, r2, l2 = pieces
    h = ROWS // 2
    return [
        (own, mb.at[:, lane : lane + 256]),
        (r1, mb.at[:, lane + 256 : lane + 512]),
        (l1, mb.at[:, lane + 512 : lane + 768]),
        (r2, mb.at[:h, lane + 768 : lane + 1024]),
        (l2, mb.at[h:, lane + 768 : lane + 1024]),
    ]


def out_kernel(sc, *refs):
    attn, conv, ws = refs[:5], refs[5:8], refs[8:14]
    part_ref, tail_ref, mb, wb, sem = refs[14:]
    spots = []
    for k, src in enumerate(weight_sources(ws)):
        row = pl.multiple_of((sc[k] // 4) * ZB, ZB)
        lane = pl.multiple_of(sc[16 + k] * 256, 256)
        spots.append((src.at[:, :256], wb.at[pl.ds(row, ZB), pl.ds(lane, 256)]))
        lane = pl.multiple_of(sc[16 + k] * 256 + 1024, 256)
        spots.append((src.at[:, 256:], wb.at[pl.ds(row, ZB), pl.ds(lane, 256)]))
    spots += mixer_spots(attn, mb, 0) + mixer_spots(conv + (None, None), mb, 1024)[:3]
    copies = [pltpu.make_async_copy(a, b, sem.at[i]) for i, (a, b) in enumerate(spots)]
    start(copies)
    wait(copies)
    for i in range(ROWS // 256):
        rows = slice(i * 256, i * 256 + 256)
        part_ref[rows, :] = lax.dot_general(
            mb[rows, :SOON], wb[:, :SOON], (((1,), (1,)), ((), ())), preferred_element_type=F32
        )
    tail_ref[...] = wb[:, SOON:]


def finish_kernel(part_ref, tail_ref, top_ref, bottom_ref, out_ref, stat_ref):
    h = ROWS // 2
    for i, ref in enumerate((top_ref, bottom_ref)):
        s = part_ref[i * h : i * h + h, :] + lax.dot_general(
            ref[...], tail_ref[...], (((1,), (1,)), ((), ())), preferred_element_type=F32
        )
        out_ref[i * h : i * h + h, :] = s
        mean = jnp.sum(s, -1, keepdims=True) * (1.0 / PART)
        d = s - mean
        second = jnp.sum(d * d, -1, keepdims=True)
        for j in range(h // 128):
            part = slice(j * 128, j * 128 + 128)
            rows = slice(i * h + j * 128, i * h + j * 128 + 128)
            stat_ref[0:1, rows] = jnp.broadcast_to(mean[part], (128, 128)).T[0:1]
            stat_ref[1:2, rows] = jnp.broadcast_to(second[part], (128, 128)).T[0:1]


def norm_kernel(sum_ref, s0, s1, s2, s3, gain_ref, out_ref, buf, sem):
    parts = (s0, s1, s2, s3)
    gain = gain_ref[...]

    copies = []
    for i in range(ROWS // 128):
        rows = slice(i * 128, i * 128 + 128)
        means = [p[0:1, rows] for p in parts]
        mean = (means[0] + means[1] + means[2] + means[3]) * 0.25
        second = sum(p[1:2, rows] for p in parts)
        second = second + PART * sum((m - mean) * (m - mean) for m in means)
        scale = lax.rsqrt(second * (1.0 / WIDTH) + EPS)
        mean = jnp.broadcast_to(mean, (128, 128)).T[:, 0:1]
        scale = jnp.broadcast_to(scale, (128, 128)).T[:, 0:1]
        buf[rows, :] = ((sum_ref[rows, :] - mean) * scale * gain).astype(BF16)
        copies.append(pltpu.make_async_copy(buf.at[rows, :], out_ref.at[rows, :], sem.at[i]))
        copies[-1].start()
    wait(copies)


def pack_kernel(*refs):
    out = refs[-1]
    at = 0
    for r in refs[:-1]:
        out[:, at : at + r.shape[1]] = r[...]
        at += r.shape[1]


def cost(flops, read):
    return pl.CostEstimate(flops=int(flops), bytes_accessed=int(read), transcendentals=0)


def params(mib):
    return pltpu.CompilerParams(vmem_limit_bytes=mib * 1024 * 1024)


def rope_tables(first_row):
    half = HEAD // 2
    inverse = THETA ** (-jnp.arange(0, half, 2, dtype=F32) / half)
    count = EXT // GRID
    row = (first_row + jnp.arange(count, dtype=jnp.int32)).astype(F32)
    column = jnp.arange(GRID, dtype=jnp.int32).astype(F32)
    place = jnp.concatenate([row, column])
    angles = place[:, None] * jnp.concatenate([inverse] * 4)
    return jnp.cos(angles), jnp.sin(angles)


def body(
    tokens,
    query_weight,
    key_projection,
    value_projection,
    conv_in_weight,
    conv_gate_out,
    conv_gate_in,
    conv_taps,
    head_sink_logit,
    out_attn_weight,
    out_conv_weight,
    out_gain,
):
    s = lax.axis_index("sp")
    x = lax.axis_index("tp")
    z, core = s // 8, s % 2
    sign = 2 * core - 1
    steps = jnp.array([0, 1, 2, 3, 4, -1, -2, -3], jnp.int32)
    turns = jnp.array([0, -1, 1, 2], jnp.int32)
    plane_of = (z + sign * steps + 8) % 8
    apart = (plane_of - x) % 4
    slot = jnp.where(apart == 3, 1, jnp.where(apart == 0, 0, apart + 1))
    sc = jnp.concatenate(
        [plane_of, (x + turns + 4) % 4, jnp.full((4,), s, jnp.int32), slot]
    ).astype(jnp.int32)

    toks = x_pass(tokens, 1)
    up = [(i, i + 1) for i in range(63)]
    down = [(i + 1, i) for i in range(63)]
    low = lax.ppermute(tokens[ROWS - WINDOW :], "sp", up)
    high = lax.ppermute(tokens[:WINDOW], "sp", down)
    halos = x_pass(jnp.concatenate([low, high], 0), -1)
    stacked = jnp.concatenate([out_attn_weight.T, out_conv_weight.T], 1)
    stacked = lax.ppermute(stacked, ("sp", "tp"), spread_out_weights())

    packed = pl.pallas_call(
        pack_kernel,
        out_shape=jax.ShapeDtypeStruct((32, QKV + CNV + OUT), BF16),
        in_specs=[VMEM] * 7,
        out_specs=VMEM,
        cost_estimate=cost(1e6, 3e5),
    )(
        key_projection,
        value_projection,
        query_weight,
        conv_in_weight,
        conv_gate_in,
        conv_gate_out,
        stacked,
    )
    planes = [[chip(z, y, c) for y in range(4) for c in range(2)] for z in range(8)]
    plane = lax.all_gather(packed, "sp", axis=0, tiled=True, axis_index_groups=planes)
    w_qkv = z_ring(plane[:, :QKV])
    w_cnv = z_ring(plane[:, QKV : QKV + CNV])
    w_out = z_ring(plane[:, QKV + CNV :])

    cosine, sine = rope_tables(s * (ROWS // GRID) - WINDOW // GRID)

    mixer = jax.ShapeDtypeStruct((ROWS, 256), BF16)
    kv, query = pl.pallas_call(
        project_kernel,
        out_shape=(jax.ShapeDtypeStruct((EXT, 256), BF16), mixer),
        in_specs=[SMEM] + [ANY] * 14 + [VMEM] * 2,
        out_specs=(VMEM,) * 2,
        scratch_shapes=[
            pltpu.VMEM((EXT, WIDTH), BF16),
            pltpu.VMEM((WIDTH, QKV), BF16),
            pltpu.SemaphoreType.DMA((24,)),
        ],
        compiler_params=params(16),
        cost_estimate=cost(2e9, 6e6),
    )(sc, *toks, *halos, *w_qkv, cosine, sine)
    attention = pl.pallas_call(
        attn_kernel,
        out_shape=mixer,
        in_specs=[SMEM, SMEM] + [VMEM] * 2,
        out_specs=VMEM,
        compiler_params=params(10),
        cost_estimate=cost(2e9, 2e6),
    )(sc, head_sink_logit, kv, query)
    conv = pl.pallas_call(
        conv_kernel,
        out_shape=mixer,
        in_specs=[SMEM] + [ANY] * 14 + [VMEM],
        out_specs=VMEM,
        scratch_shapes=[
            pltpu.VMEM((CONV_ROWS, WIDTH), BF16),
            pltpu.VMEM((WIDTH, CNV), BF16),
            pltpu.VMEM((CONV_ROWS, 256), F32),
            pltpu.SemaphoreType.DMA((24,)),
        ],
        compiler_params=params(18),
        cost_estimate=cost(3e9, 8e6),
    )(sc, *toks, *halos, *w_cnv, conv_taps)
    attn_all = x_ring(attention)
    conv_all = x_ring(conv)
    partial, tail = pl.pallas_call(
        out_kernel,
        out_shape=(
            jax.ShapeDtypeStruct((ROWS, PART), F32),
            jax.ShapeDtypeStruct((PART, WIDTH - SOON), BF16),
        ),
        in_specs=[SMEM] + [ANY] * 14,
        out_specs=(VMEM, VMEM),
        scratch_shapes=[
            pltpu.VMEM((ROWS, WIDTH), BF16),
            pltpu.VMEM((PART, WIDTH), BF16),
            pltpu.SemaphoreType.DMA((24,)),
        ],
        compiler_params=params(16),
        cost_estimate=cost(1.4e9, 6e6),
    )(sc, *attn_all, *conv_all[:3], *w_out)
    summed, stats = pl.pallas_call(
        finish_kernel,
        out_shape=(
            jax.ShapeDtypeStruct((ROWS, PART), F32),
            jax.ShapeDtypeStruct((2, ROWS), F32),
        ),
        in_specs=[VMEM] * 4,
        out_specs=(VMEM, VMEM),
        compiler_params=params(14),
        cost_estimate=cost(4e8, 4e6),
    )(partial, tail, *conv_all[3:])
    others = []
    for d in (1, -1, 2):
        others.append(lax.ppermute(stats, "tp", turn(d)))
    return pl.pallas_call(
        norm_kernel,
        out_shape=jax.ShapeDtypeStruct((ROWS, PART), BF16),
        in_specs=[VMEM] * 6,
        out_specs=ANY,
        scratch_shapes=[
            pltpu.VMEM((ROWS, PART), BF16),
            pltpu.SemaphoreType.DMA((ROWS // 128,)),
        ],
        compiler_params=params(10),
        cost_estimate=cost(4e6, 3e6),
    )(summed, stats, *others, out_gain.reshape(1, PART))


def solution(mesh):
    return jax.shard_map(
        body,
        mesh=mesh,
        in_specs=(
            P("sp", "tp"),
            P("sp", "tp"),
            P("sp", "tp"),
            P("sp", "tp"),
            P("sp", "tp"),
            P("sp", "tp"),
            P("sp", "tp"),
            P(None, "tp"),
            P("tp"),
            P("tp", "sp"),
            P("tp", "sp"),
            P("tp"),
        ),
        out_specs=P("sp", "tp"),
        check_vma=False,
    )
```

```python
import jax
import jax.numpy as jnp
from jax import lax
from jax.experimental import pallas as pl
from jax.experimental.pallas import tpu as pltpu
from jax.sharding import PartitionSpec as P


HEAD = 128
WINDOW = 128
GRID = 64
NEG_BIG = -1e30
THETA = 10000.0
EPS = 1e-05

ROWS = 768
EXT = ROWS + 256
WIDTH = 2048
PART = 512
QKV = 512
CNV = 768
OUT = 512
ZB = 256


ANY = pl.BlockSpec(memory_space=pl.ANY)
SMEM = pl.BlockSpec(memory_space=pltpu.SMEM)
VMEM = pl.BlockSpec(memory_space=pltpu.VMEM)
F32 = jnp.float32
BF16 = jnp.bfloat16


def chip(z, y, c):
    return ((z % 8) * 4 + y % 4) * 2 + c


def up_down():
    return [
        (chip(z, y, c), chip(z + 1 - 2 * c, y, c))
        for z in range(8)
        for y in range(4)
        for c in range(2)
    ]


def partner():
    return [(i, i ^ 1) for i in range(64)]


def turn(d):
    return [(i, (i + d) % 4) for i in range(4)]


def spread_out_weights():
    pairs = []
    for z in range(8):
        for y in range(4):
            for c in range(2):
                for t in range(4):
                    target = chip((z % 2) * 4 + t, y, c) * 4 + z // 2
                    pairs.append((chip(z, y, c) * 4 + t, target))
    return pairs


def x_ring(block):
    h = block.shape[0] // 2
    r1 = lax.ppermute(block, "tp", turn(1))
    l1 = lax.ppermute(block, "tp", turn(-1))
    r2 = lax.ppermute(r1[:h], "tp", turn(1))
    l2 = lax.ppermute(l1[h:], "tp", turn(-1))
    return [block, r1, l1, r2, l2]


def x_pass(block, way):
    r1 = lax.ppermute(block, "tp", turn(1))
    l1 = lax.ppermute(block, "tp", turn(-1))
    far = lax.ppermute(r1 if way == 1 else l1, "tp", turn(way))
    return [block, r1, l1, far]


def z_ring(block):
    got = [block]
    for _ in range(1, 5):
        got.append(lax.ppermute(got[-1], "sp", up_down()))
    e = lax.ppermute(jnp.concatenate(got[1:4], 0), "sp", partner())
    return got + [e]


def start(copies):
    for c in copies:
        c.start()


def wait(copies):
    for c in copies:
        c.wait()


def place_kernel(*refs):
    toks, halos, out, sem = refs[:4], refs[4:8], refs[8], refs[9]
    copies = []
    for i in range(4):
        lanes = slice(i * PART, (i + 1) * PART)
        spots = (
            (halos[i].at[:WINDOW, :], slice(0, WINDOW)),
            (toks[i], slice(WINDOW, WINDOW + ROWS)),
            (halos[i].at[WINDOW:, :], slice(WINDOW + ROWS, EXT)),
        )
        for j, (src, rows) in enumerate(spots):
            copies.append(pltpu.make_async_copy(src, out.at[rows, lanes], sem.at[3 * i + j]))
    start(copies)
    wait(copies)


def weight_sources(ws):
    block, m1, m2, m3, m4, e = ws
    return [block, m1, m2, m3, m4] + [e.at[pl.ds(k * ZB, ZB), :] for k in range(3)]


def project(sc, tb, rows, ws, lanes):
    total = None
    for k, w in enumerate(weight_sources(ws)):
        part = tb[rows, pl.ds(pl.multiple_of(sc[24 + k] * ZB, ZB), ZB)]
        part = jnp.dot(part, w[:, lanes], preferred_element_type=F32)
        total = part if total is None else total + part
    return total


def rotate(u, cos, sin, even):
    turned = jnp.where(even, -pltpu.roll(u, 96, 1), pltpu.roll(u, 32, 1))
    return u * cos + turned * sin


def spread_table(ref, first, count):
    by_row = lax.broadcasted_iota(jnp.int32, (GRID, HEAD), 1) < HEAD // 2
    column = ref[16 : 16 + GRID, :]
    groups = [
        jnp.where(by_row, jnp.broadcast_to(ref[g : g + 1, :], (GRID, HEAD)), column)
        for g in range(first, first + count)
    ]
    return jnp.concatenate(groups, 0)


def project_kernel(sc, tb, *refs):
    ws, (cos_ref, sin_ref, kv_ref, q_ref) = refs[:6], refs[6:]
    n = 256
    even = (lax.broadcasted_iota(jnp.int32, (n, HEAD), 1) // 32) % 2 == 0
    for i in range(EXT // n):
        rows = slice(i * n, i * n + n)
        u = project(sc, tb, rows, ws, slice(0, 256))
        cos, sin = (spread_table(t, i * n // GRID, n // GRID) for t in (cos_ref, sin_ref))
        kv_ref[rows, :HEAD] = rotate(u[:, :HEAD], cos, sin, even).astype(BF16)
        kv_ref[rows, HEAD:] = u[:, HEAD:].astype(BF16)
    for i in range(ROWS // n):
        first = i * n + WINDOW
        u = project(sc, tb, slice(first, first + n), ws, slice(256, 512))
        cos, sin = (spread_table(t, first // GRID, n // GRID) for t in (cos_ref, sin_ref))
        for h in range(2):
            lanes = slice(h * HEAD, (h + 1) * HEAD)
            q_ref[i * n : i * n + n, lanes] = rotate(u[:, lanes], cos, sin, even).astype(BF16)


def attn_kernel(sc, sink, kb, q_ref, out_ref):
    place = sc[12]
    two = 2 * WINDOW
    row = lax.broadcasted_iota(jnp.int32, (two, WINDOW), 0) % WINDOW
    col = lax.broadcasted_iota(jnp.int32, (two, WINDOW), 1)
    sinks = jnp.where(
        lax.broadcasted_iota(jnp.int32, (two, 1), 0) < WINDOW, sink[0], sink[1]
    )
    count = ROWS // WINDOW
    for n in range(count):
        left, right = col >= row, col <= row
        if n == 0:
            left = left & (col >= jnp.where(place == 0, WINDOW, 0))
        if n == count - 1:
            right = right & (col < jnp.where(place == 63, 0, WINDOW))
        keys = slice(n * WINDOW, (n + 3) * WINDOW)
        rows = slice(n * WINDOW, (n + 1) * WINDOW)
        k, v = kb[keys, :HEAD], kb[keys, HEAD:]
        q = jnp.concatenate([q_ref[rows, :HEAD], q_ref[rows, HEAD:]], 0)
        s = lax.dot_general(q, k, (((1,), (1,)), ((), ())), preferred_element_type=F32)
        s = s * HEAD ** (-0.5)
        s0 = jnp.where(left, s[:, :WINDOW], NEG_BIG)
        s1 = s[:, WINDOW:two]
        s2 = jnp.where(right, s[:, two:], NEG_BIG)
        top = jnp.maximum(jnp.maximum(s0, s1), s2)
        top = jnp.maximum(jnp.max(top, -1, keepdims=True), sinks)
        w0, w1, w2 = jnp.exp(s0 - top), jnp.exp(s1 - top), jnp.exp(s2 - top)
        total = jnp.sum(w0 + w1 + w2, -1, keepdims=True) + jnp.exp(sinks - top)
        inverse = 1.0 / total
        probs = jnp.concatenate([w0 * inverse, w1 * inverse, w2 * inverse], 1).astype(BF16)
        o = jnp.dot(probs, v, preferred_element_type=F32).astype(BF16)
        out_ref[rows, :HEAD] = o[:WINDOW]
        out_ref[rows, HEAD:] = o[WINDOW:]


CONV_ROWS = ROWS + 32


def conv_kernel(sc, tb, *refs):
    ws, (taps_ref, out_ref, sb) = refs[:6], refs[6:]
    for lo, hi in ((0, 272), (272, 544), (544, 800)):
        both = project(sc, tb, slice(lo + 112, hi + 112), ws, slice(0, 512))
        sb[lo:hi, :] = (both[:, 256:] * both[:, :256]).astype(BF16).astype(F32)
    taps = taps_ref[...].astype(F32)
    for i in range(ROWS // 256):
        r = i * 256
        gate = project(sc, tb, slice(r + WINDOW, r + WINDOW + 256), ws, slice(512, 768))
        s = sb[r + 8 : r + 280, :]
        before = pltpu.roll(s, 1, 0)[8:264]
        after = pltpu.roll(s, 271, 0)[8:264]
        conv = before * taps[0:1] + s[8:264] * taps[1:2] + after * taps[2:3]
        out_ref[r : r + 256, :] = (gate * conv).astype(BF16)


SOON = 1792


def mixer_spots(pieces, mb, lane):
    own, r1, l1, r2, l2 = pieces
    h = ROWS // 2
    return [
        (own, mb.at[:, lane : lane + 256]),
        (r1, mb.at[:, lane + 256 : lane + 512]),
        (l1, mb.at[:, lane + 512 : lane + 768]),
        (r2, mb.at[:h, lane + 768 : lane + 1024]),
        (l2, mb.at[h:, lane + 768 : lane + 1024]),
    ]


def out_kernel(sc, *refs):
    attn, conv, ws = refs[:5], refs[5:8], refs[8:14]
    part_ref, tail_ref, mb, wb, sem = refs[14:]
    spots = []
    for k, src in enumerate(weight_sources(ws)):
        row = pl.multiple_of((sc[k] // 4) * ZB, ZB)
        lane = pl.multiple_of(sc[16 + k] * 256, 256)
        spots.append((src.at[:, :256], wb.at[pl.ds(row, ZB), pl.ds(lane, 256)]))
        lane = pl.multiple_of(sc[16 + k] * 256 + 1024, 256)
        spots.append((src.at[:, 256:], wb.at[pl.ds(row, ZB), pl.ds(lane, 256)]))
    spots += mixer_spots(attn, mb, 0) + mixer_spots(conv + (None, None), mb, 1024)[:3]
    copies = [pltpu.make_async_copy(a, b, sem.at[i]) for i, (a, b) in enumerate(spots)]
    start(copies)
    wait(copies)
    for i in range(ROWS // 256):
        rows = slice(i * 256, i * 256 + 256)
        part_ref[rows, :] = lax.dot_general(
            mb[rows, :SOON], wb[:, :SOON], (((1,), (1,)), ((), ())), preferred_element_type=F32
        )
    tail_ref[...] = wb[:, SOON:]


def finish_kernel(part_ref, tail_ref, top_ref, bottom_ref, out_ref, stat_ref):
    h = ROWS // 2
    for i, ref in enumerate((top_ref, bottom_ref)):
        s = part_ref[i * h : i * h + h, :] + lax.dot_general(
            ref[...], tail_ref[...], (((1,), (1,)), ((), ())), preferred_element_type=F32
        )
        out_ref[i * h : i * h + h, :] = s
        mean = jnp.sum(s, -1, keepdims=True) * (1.0 / PART)
        d = s - mean
        second = jnp.sum(d * d, -1, keepdims=True)
        for j in range(h // 128):
            part = slice(j * 128, j * 128 + 128)
            rows = slice(i * h + j * 128, i * h + j * 128 + 128)
            stat_ref[0:1, rows] = jnp.broadcast_to(mean[part], (128, 128)).T[0:1]
            stat_ref[1:2, rows] = jnp.broadcast_to(second[part], (128, 128)).T[0:1]


def norm_kernel(sum_ref, s0, s1, s2, s3, gain_ref, out_ref, buf, sem):
    parts = (s0, s1, s2, s3)
    gain = gain_ref[...]

    copies = []
    for i in range(ROWS // 128):
        rows = slice(i * 128, i * 128 + 128)
        means = [p[0:1, rows] for p in parts]
        mean = (means[0] + means[1] + means[2] + means[3]) * 0.25
        second = sum(p[1:2, rows] for p in parts)
        second = second + PART * sum((m - mean) * (m - mean) for m in means)
        scale = lax.rsqrt(second * (1.0 / WIDTH) + EPS)
        mean = jnp.broadcast_to(mean, (128, 128)).T[:, 0:1]
        scale = jnp.broadcast_to(scale, (128, 128)).T[:, 0:1]
        buf[rows, :] = ((sum_ref[rows, :] - mean) * scale * gain).astype(BF16)
        copies.append(pltpu.make_async_copy(buf.at[rows, :], out_ref.at[rows, :], sem.at[i]))
        copies[-1].start()
    wait(copies)


def pack_kernel(*refs):
    out = refs[-1]
    at = 0
    for r in refs[:-1]:
        out[:, at : at + r.shape[1]] = r[...]
        at += r.shape[1]


def cost(flops, read):
    return pl.CostEstimate(flops=int(flops), bytes_accessed=int(read), transcendentals=0)


def params(mib):
    return pltpu.CompilerParams(vmem_limit_bytes=mib * 1024 * 1024)


def rope_tables(first_row):
    half = HEAD // 2
    inverse = THETA ** (-jnp.arange(0, half, 2, dtype=F32) / half)
    count = EXT // GRID
    row = (first_row + jnp.arange(count, dtype=jnp.int32)).astype(F32)
    column = jnp.arange(GRID, dtype=jnp.int32).astype(F32)
    place = jnp.concatenate([row, column])
    angles = place[:, None] * jnp.concatenate([inverse] * 4)
    return jnp.cos(angles), jnp.sin(angles)


def body(
    tokens,
    query_weight,
    key_projection,
    value_projection,
    conv_in_weight,
    conv_gate_out,
    conv_gate_in,
    conv_taps,
    head_sink_logit,
    out_attn_weight,
    out_conv_weight,
    out_gain,
):
    s = lax.axis_index("sp")
    x = lax.axis_index("tp")
    z, core = s >> 3, s & 1
    sign = 2 * core - 1
    steps = jnp.array([0, 1, 2, 3, 4, -1, -2, -3], jnp.int32)
    plane_of = (z + sign * steps) & 7
    apart = (jnp.concatenate([plane_of, plane_of >> 1]) - x) & 3
    slot = jnp.where(apart == 3, 1, jnp.where(apart == 0, 0, apart + 1))
    sc = jnp.concatenate(
        [plane_of, jnp.full((8,), s, jnp.int32), slot[:8], 2 * slot[8:] + (plane_of & 1)]
    ).astype(jnp.int32)

    toks = x_pass(tokens, 1)
    up = [(i, i + 1) for i in range(63)]
    down = [(i + 1, i) for i in range(63)]
    low = lax.ppermute(tokens[ROWS - WINDOW :], "sp", up)
    high = lax.ppermute(tokens[:WINDOW], "sp", down)
    halos = x_pass(jnp.concatenate([low, high], 0), -1)
    stacked = jnp.concatenate([out_attn_weight.T, out_conv_weight.T], 1)
    stacked = lax.ppermute(stacked, ("sp", "tp"), spread_out_weights())

    packed = pl.pallas_call(
        pack_kernel,
        out_shape=jax.ShapeDtypeStruct((32, QKV + CNV + OUT), BF16),
        in_specs=[VMEM] * 7,
        out_specs=VMEM,
        cost_estimate=cost(1e6, 3e5),
    )(
        key_projection,
        value_projection,
        query_weight,
        conv_in_weight,
        conv_gate_in,
        conv_gate_out,
        stacked,
    )
    planes = [[chip(z, y, c) for y in range(4) for c in range(2)] for z in range(8)]
    plane = lax.all_gather(packed, "sp", axis=0, tiled=True, axis_index_groups=planes)
    w_qkv = z_ring(plane[:, :QKV])
    w_cnv = z_ring(plane[:, QKV : QKV + CNV])
    w_out = z_ring(plane[:, QKV + CNV :])

    cosine, sine = rope_tables(s * (ROWS // GRID) - WINDOW // GRID)

    mixer = jax.ShapeDtypeStruct((ROWS, 256), BF16)
    placed = pl.pallas_call(
        place_kernel,
        out_shape=jax.ShapeDtypeStruct((EXT, WIDTH), BF16),
        in_specs=[ANY] * 8,
        out_specs=VMEM,
        scratch_shapes=[pltpu.SemaphoreType.DMA((12,))],
        compiler_params=params(8),
        cost_estimate=cost(1e6, 8e6),
    )(*toks, *halos)
    kv, query = pl.pallas_call(
        project_kernel,
        out_shape=(jax.ShapeDtypeStruct((EXT, 256), BF16), mixer),
        in_specs=[SMEM] + [VMEM] * 9,
        out_specs=(VMEM,) * 2,
        compiler_params=params(16),
        cost_estimate=cost(2e9, 6e6),
    )(sc, placed, *w_qkv, cosine, sine)
    attention = pl.pallas_call(
        attn_kernel,
        out_shape=mixer,
        in_specs=[SMEM, SMEM] + [VMEM] * 2,
        out_specs=VMEM,
        compiler_params=params(10),
        cost_estimate=cost(2e9, 2e6),
    )(sc, head_sink_logit, kv, query)
    conv = pl.pallas_call(
        conv_kernel,
        out_shape=mixer,
        in_specs=[SMEM] + [VMEM] * 8,
        out_specs=VMEM,
        scratch_shapes=[pltpu.VMEM((CONV_ROWS, 256), F32)],
        compiler_params=params(18),
        cost_estimate=cost(3e9, 8e6),
    )(sc, placed, *w_cnv, conv_taps)
    attn_all = x_ring(attention)
    conv_all = x_ring(conv)
    partial, tail = pl.pallas_call(
        out_kernel,
        out_shape=(
            jax.ShapeDtypeStruct((ROWS, PART), F32),
            jax.ShapeDtypeStruct((PART, WIDTH - SOON), BF16),
        ),
        in_specs=[SMEM] + [ANY] * 14,
        out_specs=(VMEM, VMEM),
        scratch_shapes=[
            pltpu.VMEM((ROWS, WIDTH), BF16),
            pltpu.VMEM((PART, WIDTH), BF16),
            pltpu.SemaphoreType.DMA((24,)),
        ],
        compiler_params=params(16),
        cost_estimate=cost(1.4e9, 6e6),
    )(sc, *attn_all, *conv_all[:3], *w_out)
    summed, stats = pl.pallas_call(
        finish_kernel,
        out_shape=(
            jax.ShapeDtypeStruct((ROWS, PART), F32),
            jax.ShapeDtypeStruct((2, ROWS), F32),
        ),
        in_specs=[VMEM] * 4,
        out_specs=(VMEM, VMEM),
        compiler_params=params(14),
        cost_estimate=cost(4e8, 4e6),
    )(partial, tail, *conv_all[3:])
    others = []
    for d in (1, -1, 2):
        others.append(lax.ppermute(stats, "tp", turn(d)))
    return pl.pallas_call(
        norm_kernel,
        out_shape=jax.ShapeDtypeStruct((ROWS, PART), BF16),
        in_specs=[VMEM] * 6,
        out_specs=ANY,
        scratch_shapes=[
            pltpu.VMEM((ROWS, PART), BF16),
            pltpu.SemaphoreType.DMA((ROWS // 128,)),
        ],
        compiler_params=params(10),
        cost_estimate=cost(4e6, 3e6),
    )(summed, stats, *others, out_gain.reshape(1, PART))


def solution(mesh):
    return jax.shard_map(
        body,
        mesh=mesh,
        in_specs=(
            P("sp", "tp"),
            P("sp", "tp"),
            P("sp", "tp"),
            P("sp", "tp"),
            P("sp", "tp"),
            P("sp", "tp"),
            P("sp", "tp"),
            P(None, "tp"),
            P("tp"),
            P("tp", "sp"),
            P("tp", "sp"),
            P("tp"),
        ),
        out_specs=P("sp", "tp"),
        check_vma=False,
    )
```

```python
import jax
import jax.numpy as jnp
from jax import lax
from jax.experimental import pallas as pl
from jax.experimental.pallas import tpu as pltpu
from jax.sharding import PartitionSpec as P


HEAD = 128
WINDOW = 128
GRID = 64
NEG_BIG = -1e30
THETA = 10000.0
EPS = 1e-05

ROWS = 768
EXT = ROWS + 256
WIDTH = 2048
PART = 512
QKV = 512
CNV = 768
OUT = 512
ZB = 256


ANY = pl.BlockSpec(memory_space=pl.ANY)
SMEM = pl.BlockSpec(memory_space=pltpu.SMEM)
VMEM = pl.BlockSpec(memory_space=pltpu.VMEM)
F32 = jnp.float32
BF16 = jnp.bfloat16


def chip(z, y, c):
    return ((z % 8) * 4 + y % 4) * 2 + c


def up_down():
    return [
        (chip(z, y, c), chip(z + 1 - 2 * c, y, c))
        for z in range(8)
        for y in range(4)
        for c in range(2)
    ]


def partner():
    return [(i, i ^ 1) for i in range(64)]


def next_chip():
    return [(i, i + 1) for i in range(1, 63, 2)] + [(i, i - 1) for i in range(2, 64, 2)]


def turn(d):
    return [(i, (i + d) % 4) for i in range(4)]


def spread_out_weights():
    pairs = []
    for z in range(8):
        for y in range(4):
            for c in range(2):
                for t in range(4):
                    target = chip((z % 2) * 4 + t, y, c) * 4 + z // 2
                    pairs.append((chip(z, y, c) * 4 + t, target))
    return pairs


def x_ring(block):
    h = block.shape[0] // 2
    r1 = lax.ppermute(block, "tp", turn(1))
    l1 = lax.ppermute(block, "tp", turn(-1))
    r2 = lax.ppermute(r1[:h], "tp", turn(1))
    l2 = lax.ppermute(l1[h:], "tp", turn(-1))
    return [block, r1, l1, r2, l2]


def x_pass(block, way):
    r1 = lax.ppermute(block, "tp", turn(1))
    l1 = lax.ppermute(block, "tp", turn(-1))
    far = lax.ppermute(r1 if way == 1 else l1, "tp", turn(way))
    return [block, r1, l1, far]


def z_ring(block):
    got = [block]
    for _ in range(1, 5):
        got.append(lax.ppermute(got[-1], "sp", up_down()))
    e = lax.ppermute(jnp.concatenate(got[1:4], 0), "sp", partner())
    return got + [e]


def start(copies):
    for c in copies:
        c.start()


def wait(copies):
    for c in copies:
        c.wait()


def place_kernel(sc, *refs):
    toks, halos, out, sem = refs[:4], refs[4:8], refs[8], refs[9]
    core = sc[8] & 1
    inner = pl.multiple_of((1 - core) * (EXT - WINDOW), WINDOW)
    outer = pl.multiple_of(core * (EXT - WINDOW), WINDOW)
    copies = []
    for i in range(4):
        lanes = slice(i * PART, (i + 1) * PART)
        spots = (
            (halos[i].at[:WINDOW, :], out.at[pl.ds(inner, WINDOW), lanes]),
            (toks[i], out.at[WINDOW : WINDOW + ROWS, lanes]),
            (halos[i].at[WINDOW:, :], out.at[pl.ds(outer, WINDOW), lanes]),
        )
        for j, (src, dst) in enumerate(spots):
            copies.append(pltpu.make_async_copy(src, dst, sem.at[3 * i + j]))
    start(copies)
    wait(copies)


def weight_sources(ws):
    block, m1, m2, m3, m4, e = ws
    return [block, m1, m2, m3, m4] + [e.at[pl.ds(k * ZB, ZB), :] for k in range(3)]


def project(sc, tb, rows, ws, lanes):
    total = None
    for k, w in enumerate(weight_sources(ws)):
        part = tb[rows, pl.ds(pl.multiple_of(sc[24 + k] * ZB, ZB), ZB)]
        part = jnp.dot(part, w[:, lanes], preferred_element_type=F32)
        total = part if total is None else total + part
    return total


def rotate(u, cos, sin, even):
    turned = jnp.where(even, -pltpu.roll(u, 96, 1), pltpu.roll(u, 32, 1))
    return u * cos + turned * sin


def spread_table(ref, first, count):
    by_row = lax.broadcasted_iota(jnp.int32, (GRID, HEAD), 1) < HEAD // 2
    column = ref[16 : 16 + GRID, :]
    groups = [
        jnp.where(by_row, jnp.broadcast_to(ref[g : g + 1, :], (GRID, HEAD)), column)
        for g in range(first, first + count)
    ]
    return jnp.concatenate(groups, 0)


def project_kernel(sc, tb, *refs):
    ws, (cos_ref, sin_ref, kv_ref, q_ref) = refs[:6], refs[6:]
    n = 256
    even = (lax.broadcasted_iota(jnp.int32, (n, HEAD), 1) // 32) % 2 == 0
    for i in range(EXT // n):
        rows = slice(i * n, i * n + n)
        u = project(sc, tb, rows, ws, slice(0, 256))
        cos, sin = (spread_table(t, i * n // GRID, n // GRID) for t in (cos_ref, sin_ref))
        kv_ref[rows, :HEAD] = rotate(u[:, :HEAD], cos, sin, even).astype(BF16)
        kv_ref[rows, HEAD:] = u[:, HEAD:].astype(BF16)
    for i in range(ROWS // n):
        first = i * n + WINDOW
        u = project(sc, tb, slice(first, first + n), ws, slice(256, 512))
        cos, sin = (spread_table(t, first // GRID, n // GRID) for t in (cos_ref, sin_ref))
        for h in range(2):
            lanes = slice(h * HEAD, (h + 1) * HEAD)
            q_ref[i * n : i * n + n, lanes] = rotate(u[:, lanes], cos, sin, even).astype(BF16)


def attn_kernel(sc, sink, kb, q_ref, out_ref):
    place = sc[12]
    two = 2 * WINDOW
    row = lax.broadcasted_iota(jnp.int32, (two, WINDOW), 0) % WINDOW
    col = lax.broadcasted_iota(jnp.int32, (two, WINDOW), 1)
    sinks = jnp.where(
        lax.broadcasted_iota(jnp.int32, (two, 1), 0) < WINDOW, sink[0], sink[1]
    )
    count = ROWS // WINDOW
    for n in range(count):
        left, right = col >= row, col <= row
        if n == 0:
            left = left & (col >= jnp.where(place == 0, WINDOW, 0))
        if n == count - 1:
            right = right & (col < jnp.where(place == 63, 0, WINDOW))
        keys = slice(n * WINDOW, (n + 3) * WINDOW)
        rows = slice(n * WINDOW, (n + 1) * WINDOW)
        k, v = kb[keys, :HEAD], kb[keys, HEAD:]
        q = jnp.concatenate([q_ref[rows, :HEAD], q_ref[rows, HEAD:]], 0)
        s = lax.dot_general(q, k, (((1,), (1,)), ((), ())), preferred_element_type=F32)
        s = s * HEAD ** (-0.5)
        s0 = jnp.where(left, s[:, :WINDOW], NEG_BIG)
        s1 = s[:, WINDOW:two]
        s2 = jnp.where(right, s[:, two:], NEG_BIG)
        top = jnp.maximum(jnp.maximum(s0, s1), s2)
        top = jnp.maximum(jnp.max(top, -1, keepdims=True), sinks)
        w0, w1, w2 = jnp.exp(s0 - top), jnp.exp(s1 - top), jnp.exp(s2 - top)
        total = jnp.sum(w0 + w1 + w2, -1, keepdims=True) + jnp.exp(sinks - top)
        inverse = 1.0 / total
        probs = jnp.concatenate([w0 * inverse, w1 * inverse, w2 * inverse], 1).astype(BF16)
        o = jnp.dot(probs, v, preferred_element_type=F32).astype(BF16)
        out_ref[rows, :HEAD] = o[:WINDOW]
        out_ref[rows, HEAD:] = o[WINDOW:]


CONV_ROWS = ROWS + 32


def conv_kernel(sc, tb, *refs):
    ws, (taps_ref, out_ref, sb) = refs[:6], refs[6:]
    for lo, hi in ((0, 272), (272, 544), (544, 800)):
        both = project(sc, tb, slice(lo + 112, hi + 112), ws, slice(0, 512))
        sb[lo:hi, :] = (both[:, 256:] * both[:, :256]).astype(BF16).astype(F32)
    taps = taps_ref[...].astype(F32)
    for i in range(ROWS // 256):
        r = i * 256
        gate = project(sc, tb, slice(r + WINDOW, r + WINDOW + 256), ws, slice(512, 768))
        s = sb[r + 8 : r + 280, :]
        before = pltpu.roll(s, 1, 0)[8:264]
        after = pltpu.roll(s, 271, 0)[8:264]
        conv = before * taps[0:1] + s[8:264] * taps[1:2] + after * taps[2:3]
        out_ref[r : r + 256, :] = (gate * conv).astype(BF16)


SOON = 1792


def mixer_spots(pieces, mb, lane):
    own, r1, l1, r2, l2 = pieces
    h = ROWS // 2
    return [
        (own, mb.at[:, lane : lane + 256]),
        (r1, mb.at[:, lane + 256 : lane + 512]),
        (l1, mb.at[:, lane + 512 : lane + 768]),
        (r2, mb.at[:h, lane + 768 : lane + 1024]),
        (l2, mb.at[h:, lane + 768 : lane + 1024]),
    ]


def out_kernel(sc, *refs):
    attn, conv, ws = refs[:5], refs[5:8], refs[8:14]
    part_ref, tail_ref, mb, wb, sem = refs[14:]
    spots = []
    for k, src in enumerate(weight_sources(ws)):
        row = pl.multiple_of((sc[k] // 4) * ZB, ZB)
        lane = pl.multiple_of(sc[16 + k] * 256, 256)
        spots.append((src.at[:, :256], wb.at[pl.ds(row, ZB), pl.ds(lane, 256)]))
        lane = pl.multiple_of(sc[16 + k] * 256 + 1024, 256)
        spots.append((src.at[:, 256:], wb.at[pl.ds(row, ZB), pl.ds(lane, 256)]))
    spots += mixer_spots(attn, mb, 0) + mixer_spots(conv + (None, None), mb, 1024)[:3]
    copies = [pltpu.make_async_copy(a, b, sem.at[i]) for i, (a, b) in enumerate(spots)]
    start(copies)
    wait(copies)
    for i in range(ROWS // 256):
        rows = slice(i * 256, i * 256 + 256)
        part_ref[rows, :] = lax.dot_general(
            mb[rows, :SOON], wb[:, :SOON], (((1,), (1,)), ((), ())), preferred_element_type=F32
        )
    tail_ref[...] = wb[:, SOON:]


def finish_kernel(part_ref, tail_ref, top_ref, bottom_ref, out_ref, stat_ref):
    h = ROWS // 2
    for i, ref in enumerate((top_ref, bottom_ref)):
        s = part_ref[i * h : i * h + h, :] + lax.dot_general(
            ref[...], tail_ref[...], (((1,), (1,)), ((), ())), preferred_element_type=F32
        )
        out_ref[i * h : i * h + h, :] = s
        mean = jnp.sum(s, -1, keepdims=True) * (1.0 / PART)
        d = s - mean
        second = jnp.sum(d * d, -1, keepdims=True)
        for j in range(h // 128):
            part = slice(j * 128, j * 128 + 128)
            rows = slice(i * h + j * 128, i * h + j * 128 + 128)
            stat_ref[0:1, rows] = jnp.broadcast_to(mean[part], (128, 128)).T[0:1]
            stat_ref[1:2, rows] = jnp.broadcast_to(second[part], (128, 128)).T[0:1]


def norm_kernel(sum_ref, s0, s1, s2, s3, gain_ref, out_ref, buf, sem):
    parts = (s0, s1, s2, s3)
    gain = gain_ref[...]

    copies = []
    for i in range(ROWS // 128):
        rows = slice(i * 128, i * 128 + 128)
        means = [p[0:1, rows] for p in parts]
        mean = (means[0] + means[1] + means[2] + means[3]) * 0.25
        second = sum(p[1:2, rows] for p in parts)
        second = second + PART * sum((m - mean) * (m - mean) for m in means)
        scale = lax.rsqrt(second * (1.0 / WIDTH) + EPS)
        mean = jnp.broadcast_to(mean, (128, 128)).T[:, 0:1]
        scale = jnp.broadcast_to(scale, (128, 128)).T[:, 0:1]
        buf[rows, :] = ((sum_ref[rows, :] - mean) * scale * gain).astype(BF16)
        copies.append(pltpu.make_async_copy(buf.at[rows, :], out_ref.at[rows, :], sem.at[i]))
        copies[-1].start()
    wait(copies)


def pack_kernel(*refs):
    out = refs[-1]
    at = 0
    for r in refs[:-1]:
        out[:, at : at + r.shape[1]] = r[...]
        at += r.shape[1]


def cost(flops, read):
    return pl.CostEstimate(flops=int(flops), bytes_accessed=int(read), transcendentals=0)


def params(mib):
    return pltpu.CompilerParams(vmem_limit_bytes=mib * 1024 * 1024)


def rope_tables(first_row):
    half = HEAD // 2
    inverse = THETA ** (-jnp.arange(0, half, 2, dtype=F32) / half)
    count = EXT // GRID
    row = (first_row + jnp.arange(count, dtype=jnp.int32)).astype(F32)
    column = jnp.arange(GRID, dtype=jnp.int32).astype(F32)
    place = jnp.concatenate([row, column])
    angles = place[:, None] * jnp.concatenate([inverse] * 4)
    return jnp.cos(angles), jnp.sin(angles)


def body(
    tokens,
    query_weight,
    key_projection,
    value_projection,
    conv_in_weight,
    conv_gate_out,
    conv_gate_in,
    conv_taps,
    head_sink_logit,
    out_attn_weight,
    out_conv_weight,
    out_gain,
):
    s = lax.axis_index("sp")
    x = lax.axis_index("tp")
    z, core = s >> 3, s & 1
    sign = 2 * core - 1
    steps = jnp.array([0, 1, 2, 3, 4, -1, -2, -3], jnp.int32)
    plane_of = (z + sign * steps) & 7
    apart = (jnp.concatenate([plane_of, plane_of >> 1]) - x) & 3
    slot = jnp.where(apart == 3, 1, jnp.where(apart == 0, 0, apart + 1))
    sc = jnp.concatenate(
        [plane_of, jnp.full((8,), s, jnp.int32), slot[:8], 2 * slot[8:] + (plane_of & 1)]
    ).astype(jnp.int32)

    toks = x_pass(tokens, 1)
    last = ROWS - WINDOW
    within = lax.dynamic_slice(tokens, ((1 - core) * last, 0), (WINDOW, PART))
    across = lax.dynamic_slice(tokens, (core * last, 0), (WINDOW, PART))
    within = lax.ppermute(within, "sp", partner())
    across = lax.ppermute(across, "sp", next_chip())
    halos = x_pass(jnp.concatenate([within, across], 0), -1)
    stacked = jnp.concatenate([out_attn_weight.T, out_conv_weight.T], 1)
    stacked = lax.ppermute(stacked, ("sp", "tp"), spread_out_weights())

    packed = pl.pallas_call(
        pack_kernel,
        out_shape=jax.ShapeDtypeStruct((32, QKV + CNV + OUT), BF16),
        in_specs=[VMEM] * 7,
        out_specs=VMEM,
        cost_estimate=cost(1e6, 3e5),
    )(
        key_projection,
        value_projection,
        query_weight,
        conv_in_weight,
        conv_gate_in,
        conv_gate_out,
        stacked,
    )
    planes = [[chip(z, y, c) for y in range(4) for c in range(2)] for z in range(8)]
    plane = lax.all_gather(packed, "sp", axis=0, tiled=True, axis_index_groups=planes)
    w_qkv = z_ring(plane[:, :QKV])
    own_cnv = plane[:, QKV : QKV + CNV]
    w_cnv = z_ring(own_cnv)
    w_out = z_ring(plane[:, QKV + CNV :])

    cosine, sine = rope_tables(s * (ROWS // GRID) - WINDOW // GRID)

    mixer = jax.ShapeDtypeStruct((ROWS, 256), BF16)
    placed = pl.pallas_call(
        place_kernel,
        out_shape=jax.ShapeDtypeStruct((EXT, WIDTH), BF16),
        in_specs=[SMEM] + [ANY] * 8,
        out_specs=VMEM,
        scratch_shapes=[pltpu.SemaphoreType.DMA((12,))],
        compiler_params=params(8),
        cost_estimate=cost(1e6, 8e6),
    )(sc, *toks, *halos)
    kv, query = pl.pallas_call(
        project_kernel,
        out_shape=(jax.ShapeDtypeStruct((EXT, 256), BF16), mixer),
        in_specs=[SMEM] + [VMEM] * 9,
        out_specs=(VMEM,) * 2,
        compiler_params=params(16),
        cost_estimate=cost(2e9, 6e6),
    )(sc, placed, *w_qkv, cosine, sine)
    attention = pl.pallas_call(
        attn_kernel,
        out_shape=mixer,
        in_specs=[SMEM, SMEM] + [VMEM] * 2,
        out_specs=VMEM,
        compiler_params=params(10),
        cost_estimate=cost(2e9, 2e6),
    )(sc, head_sink_logit, kv, query)
    conv = pl.pallas_call(
        conv_kernel,
        out_shape=mixer,
        in_specs=[SMEM] + [VMEM] * 8,
        out_specs=VMEM,
        scratch_shapes=[pltpu.VMEM((CONV_ROWS, 256), F32)],
        compiler_params=params(18),
        cost_estimate=cost(3e9, 8e6),
    )(sc, placed, *w_cnv, conv_taps)
    attn_all = x_ring(attention)
    conv_all = x_ring(conv)
    partial, tail = pl.pallas_call(
        out_kernel,
        out_shape=(
            jax.ShapeDtypeStruct((ROWS, PART), F32),
            jax.ShapeDtypeStruct((PART, WIDTH - SOON), BF16),
        ),
        in_specs=[SMEM] + [ANY] * 14,
        out_specs=(VMEM, VMEM),
        scratch_shapes=[
            pltpu.VMEM((ROWS, WIDTH), BF16),
            pltpu.VMEM((PART, WIDTH), BF16),
            pltpu.SemaphoreType.DMA((24,)),
        ],
        compiler_params=params(16),
        cost_estimate=cost(1.4e9, 6e6),
    )(sc, *attn_all, *conv_all[:3], *w_out)
    summed, stats = pl.pallas_call(
        finish_kernel,
        out_shape=(
            jax.ShapeDtypeStruct((ROWS, PART), F32),
            jax.ShapeDtypeStruct((2, ROWS), F32),
        ),
        in_specs=[VMEM] * 4,
        out_specs=(VMEM, VMEM),
        compiler_params=params(14),
        cost_estimate=cost(4e8, 4e6),
    )(partial, tail, *conv_all[3:])
    others = []
    for d in (1, -1, 2):
        others.append(lax.ppermute(stats, "tp", turn(d)))
    return pl.pallas_call(
        norm_kernel,
        out_shape=jax.ShapeDtypeStruct((ROWS, PART), BF16),
        in_specs=[VMEM] * 6,
        out_specs=ANY,
        scratch_shapes=[
            pltpu.VMEM((ROWS, PART), BF16),
            pltpu.SemaphoreType.DMA((ROWS // 128,)),
        ],
        compiler_params=params(10),
        cost_estimate=cost(4e6, 3e6),
    )(summed, stats, *others, out_gain.reshape(1, PART))


def solution(mesh):
    return jax.shard_map(
        body,
        mesh=mesh,
        in_specs=(
            P("sp", "tp"),
            P("sp", "tp"),
            P("sp", "tp"),
            P("sp", "tp"),
            P("sp", "tp"),
            P("sp", "tp"),
            P("sp", "tp"),
            P(None, "tp"),
            P("tp"),
            P("tp", "sp"),
            P("tp", "sp"),
            P("tp"),
        ),
        out_specs=P("sp", "tp"),
        check_vma=False,
    )
```

```python
import jax
import jax.numpy as jnp
from jax import lax
from jax.experimental import pallas as pl
from jax.experimental.pallas import tpu as pltpu
from jax.sharding import PartitionSpec as P


HEAD = 128
WINDOW = 128
GRID = 64
NEG_BIG = -1e30
THETA = 10000.0
EPS = 1e-05

ROWS = 768
EXT = ROWS + 256
WIDTH = 2048
PART = 512
QKV = 512
CNV = 768
OUT = 512
ZB = 256


ANY = pl.BlockSpec(memory_space=pl.ANY)
SMEM = pl.BlockSpec(memory_space=pltpu.SMEM)
VMEM = pl.BlockSpec(memory_space=pltpu.VMEM)
F32 = jnp.float32
BF16 = jnp.bfloat16


def chip(z, y, c):
    return ((z % 8) * 4 + y % 4) * 2 + c


def up_down():
    return [
        (chip(z, y, c), chip(z + 1 - 2 * c, y, c))
        for z in range(8)
        for y in range(4)
        for c in range(2)
    ]


def partner():
    return [(i, i ^ 1) for i in range(64)]


def next_chip():
    return [(i, i + 1) for i in range(1, 63, 2)] + [(i, i - 1) for i in range(2, 64, 2)]


def turn(d):
    return [(i, (i + d) % 4) for i in range(4)]


def spread_out_weights():
    pairs = []
    for z in range(8):
        for y in range(4):
            for c in range(2):
                for t in range(4):
                    target = chip((z % 2) * 4 + t, y, c) * 4 + z // 2
                    pairs.append((chip(z, y, c) * 4 + t, target))
    return pairs


def x_ring(block):
    h = block.shape[0] // 2
    r1 = lax.ppermute(block, "tp", turn(1))
    l1 = lax.ppermute(block, "tp", turn(-1))
    r2 = lax.ppermute(r1[:h], "tp", turn(1))
    l2 = lax.ppermute(l1[h:], "tp", turn(-1))
    return [block, r1, l1, r2, l2]


def x_pass(block, way):
    r1 = lax.ppermute(block, "tp", turn(1))
    l1 = lax.ppermute(block, "tp", turn(-1))
    far = lax.ppermute(r1 if way == 1 else l1, "tp", turn(way))
    return [block, r1, l1, far]


def z_ring(block):
    got, swapped = [block], []
    for _ in range(1, 5):
        got.append(lax.ppermute(got[-1], "sp", up_down()))
    for k in range(1, 4):
        swapped.append(lax.ppermute(got[k], "sp", partner()))
    return got + swapped


def start(copies):
    for c in copies:
        c.start()


def wait(copies):
    for c in copies:
        c.wait()


def place_kernel(sc, *refs):
    toks, halos, out, sem = refs[:4], refs[4:8], refs[8], refs[9]
    core = sc[8] & 1
    inner = pl.multiple_of((1 - core) * (EXT - WINDOW), WINDOW)
    outer = pl.multiple_of(core * (EXT - WINDOW), WINDOW)
    copies = []
    for i in range(4):
        lanes = slice(i * PART, (i + 1) * PART)
        spots = (
            (halos[i].at[:WINDOW, :], out.at[pl.ds(inner, WINDOW), lanes]),
            (toks[i], out.at[WINDOW : WINDOW + ROWS, lanes]),
            (halos[i].at[WINDOW:, :], out.at[pl.ds(outer, WINDOW), lanes]),
        )
        for j, (src, dst) in enumerate(spots):
            copies.append(pltpu.make_async_copy(src, dst, sem.at[3 * i + j]))
    start(copies)
    wait(copies)


def project(sc, tb, rows, ws, lanes):
    total = None
    for k, w in enumerate(ws):
        part = tb[rows, pl.ds(pl.multiple_of(sc[24 + k] * ZB, ZB), ZB)]
        part = jnp.dot(part, w[:, lanes], preferred_element_type=F32)
        total = part if total is None else total + part
    return total


def rotate(u, cos, sin, even):
    turned = jnp.where(even, -pltpu.roll(u, 96, 1), pltpu.roll(u, 32, 1))
    return u * cos + turned * sin


def spread_table(ref, first, count):
    by_row = lax.broadcasted_iota(jnp.int32, (GRID, HEAD), 1) < HEAD // 2
    column = ref[16 : 16 + GRID, :]
    groups = [
        jnp.where(by_row, jnp.broadcast_to(ref[pl.ds(first + g, 1), :], (GRID, HEAD)), column)
        for g in range(count)
    ]
    return jnp.concatenate(groups, 0)


def project_kernel(sc, tb, *refs):
    ws, (cos_ref, sin_ref, kv_ref, q_ref) = refs[:8], refs[8:]
    n = 256
    even = (lax.broadcasted_iota(jnp.int32, (n, HEAD), 1) // 32) % 2 == 0

    def keys(i, _):
        first = pl.multiple_of(i * n, n)
        rows = pl.ds(first, n)
        u = project(sc, tb, rows, ws, slice(0, 256))
        cos, sin = (spread_table(t, i * (n // GRID), n // GRID) for t in (cos_ref, sin_ref))
        kv_ref[rows, :HEAD] = rotate(u[:, :HEAD], cos, sin, even).astype(BF16)
        kv_ref[rows, HEAD:] = u[:, HEAD:].astype(BF16)
        return 0

    lax.fori_loop(0, EXT // n, keys, 0)

    def queries(i, _):
        rows = pl.ds(pl.multiple_of(i * n + WINDOW, WINDOW), n)
        u = project(sc, tb, rows, ws, slice(256, 512))
        place = i * (n // GRID) + WINDOW // GRID
        cos, sin = (spread_table(t, place, n // GRID) for t in (cos_ref, sin_ref))
        rows = pl.ds(pl.multiple_of(i * n, n), n)
        for h in range(2):
            lanes = slice(h * HEAD, (h + 1) * HEAD)
            q_ref[rows, lanes] = rotate(u[:, lanes], cos, sin, even).astype(BF16)
        return 0

    lax.fori_loop(0, ROWS // n, queries, 0)


def attn_kernel(sc, sink, kb, q_ref, out_ref):
    place = sc[12]
    two = 2 * WINDOW
    row = lax.broadcasted_iota(jnp.int32, (two, WINDOW), 0) % WINDOW
    col = lax.broadcasted_iota(jnp.int32, (two, WINDOW), 1)
    sinks = jnp.where(
        lax.broadcasted_iota(jnp.int32, (two, 1), 0) < WINDOW, sink[0], sink[1]
    )
    count = ROWS // WINDOW

    def block(n, left, right):
        first = pl.multiple_of(n * WINDOW, WINDOW)
        keys, rows = pl.ds(first, 3 * WINDOW), pl.ds(first, WINDOW)
        k, v = kb[keys, :HEAD], kb[keys, HEAD:]
        q = jnp.concatenate([q_ref[rows, :HEAD], q_ref[rows, HEAD:]], 0)
        s = lax.dot_general(q, k, (((1,), (1,)), ((), ())), preferred_element_type=F32)
        s = s * HEAD ** (-0.5)
        s0 = jnp.where(left, s[:, :WINDOW], NEG_BIG)
        s1 = s[:, WINDOW:two]
        s2 = jnp.where(right, s[:, two:], NEG_BIG)
        top = jnp.maximum(jnp.maximum(s0, s1), s2)
        top = jnp.maximum(jnp.max(top, -1, keepdims=True), sinks)
        w0, w1, w2 = jnp.exp(s0 - top), jnp.exp(s1 - top), jnp.exp(s2 - top)
        total = jnp.sum(w0 + w1 + w2, -1, keepdims=True) + jnp.exp(sinks - top)
        inverse = 1.0 / total
        probs = jnp.concatenate([w0 * inverse, w1 * inverse, w2 * inverse], 1).astype(BF16)
        o = jnp.dot(probs, v, preferred_element_type=F32).astype(BF16)
        out_ref[rows, :HEAD] = o[:WINDOW]
        out_ref[rows, HEAD:] = o[WINDOW:]

    def pair(i, _):
        for n in (2 * i, 2 * i + 1):
            left, right = col >= row, col <= row
            left = left & (col >= jnp.where((place == 0) & (n == 0), WINDOW, 0))
            right = right & (col < jnp.where((place == 63) & (n == count - 1), 0, WINDOW))
            block(n, left, right)
        return 0

    lax.fori_loop(0, count // 2, pair, 0)


CONV_ROWS = ROWS + 32


def conv_kernel(sc, tb, *refs):
    ws, (taps_ref, out_ref, sb) = refs[:8], refs[8:]
    for lo, hi in ((0, 272), (272, 544), (544, 800)):
        both = project(sc, tb, slice(lo + 112, hi + 112), ws, slice(0, 512))
        sb[lo:hi, :] = (both[:, 256:] * both[:, :256]).astype(BF16).astype(F32)
    taps = taps_ref[...].astype(F32)

    def mix(i, _):
        r = pl.multiple_of(i * 256, 256)
        rows = pl.ds(pl.multiple_of(r + WINDOW, WINDOW), 256)
        gate = project(sc, tb, rows, ws, slice(512, 768))
        s = sb[pl.ds(pl.multiple_of(r + 8, 8), 272), :]
        before = pltpu.roll(s, 1, 0)[8:264]
        after = pltpu.roll(s, 271, 0)[8:264]
        conv = before * taps[0:1] + s[8:264] * taps[1:2] + after * taps[2:3]
        out_ref[pl.ds(r, 256), :] = (gate * conv).astype(BF16)
        return 0

    lax.fori_loop(0, ROWS // 256, mix, 0)


SOON = 1792


def mixer_spots(pieces, mb, lane):
    own, r1, l1, r2, l2 = pieces
    h = ROWS // 2
    return [
        (own, mb.at[:, lane : lane + 256]),
        (r1, mb.at[:, lane + 256 : lane + 512]),
        (l1, mb.at[:, lane + 512 : lane + 768]),
        (r2, mb.at[:h, lane + 768 : lane + 1024]),
        (l2, mb.at[h:, lane + 768 : lane + 1024]),
    ]


def out_kernel(sc, *refs):
    attn, conv, ws = refs[:5], refs[5:8], refs[8:16]
    part_ref, tail_ref, mb, wb, sem = refs[16:]
    spots = []
    for k, src in enumerate(ws):
        row = pl.multiple_of((sc[k] // 4) * ZB, ZB)
        lane = pl.multiple_of(sc[16 + k] * 256, 256)
        spots.append((src.at[:, :256], wb.at[pl.ds(row, ZB), pl.ds(lane, 256)]))
        lane = pl.multiple_of(sc[16 + k] * 256 + 1024, 256)
        spots.append((src.at[:, 256:], wb.at[pl.ds(row, ZB), pl.ds(lane, 256)]))
    spots += mixer_spots(attn, mb, 0) + mixer_spots(conv + (None, None), mb, 1024)[:3]
    copies = [pltpu.make_async_copy(a, b, sem.at[i]) for i, (a, b) in enumerate(spots)]
    start(copies)
    wait(copies)
    for i in range(ROWS // 256):
        rows = slice(i * 256, i * 256 + 256)
        part_ref[rows, :] = lax.dot_general(
            mb[rows, :SOON], wb[:, :SOON], (((1,), (1,)), ((), ())), preferred_element_type=F32
        )
    tail_ref[...] = wb[:, SOON:]


def finish_kernel(part_ref, tail_ref, top_ref, bottom_ref, out_ref, stat_ref):
    h = ROWS // 2
    for i, ref in enumerate((top_ref, bottom_ref)):
        s = part_ref[i * h : i * h + h, :] + lax.dot_general(
            ref[...], tail_ref[...], (((1,), (1,)), ((), ())), preferred_element_type=F32
        )
        out_ref[i * h : i * h + h, :] = s
        mean = jnp.sum(s, -1, keepdims=True) * (1.0 / PART)
        d = s - mean
        second = jnp.sum(d * d, -1, keepdims=True)
        for j in range(h // 128):
            part = slice(j * 128, j * 128 + 128)
            rows = slice(i * h + j * 128, i * h + j * 128 + 128)
            stat_ref[0:1, rows] = jnp.broadcast_to(mean[part], (128, 128)).T[0:1]
            stat_ref[1:2, rows] = jnp.broadcast_to(second[part], (128, 128)).T[0:1]


def norm_kernel(sum_ref, s0, s1, s2, s3, gain_ref, out_ref, buf, sem):
    parts = (s0, s1, s2, s3)
    gain = gain_ref[...]

    copies = []
    for i in range(ROWS // 128):
        rows = slice(i * 128, i * 128 + 128)
        means = [p[0:1, rows] for p in parts]
        mean = (means[0] + means[1] + means[2] + means[3]) * 0.25
        second = sum(p[1:2, rows] for p in parts)
        second = second + PART * sum((m - mean) * (m - mean) for m in means)
        scale = lax.rsqrt(second * (1.0 / WIDTH) + EPS)
        mean = jnp.broadcast_to(mean, (128, 128)).T[:, 0:1]
        scale = jnp.broadcast_to(scale, (128, 128)).T[:, 0:1]
        buf[rows, :] = ((sum_ref[rows, :] - mean) * scale * gain).astype(BF16)
        copies.append(pltpu.make_async_copy(buf.at[rows, :], out_ref.at[rows, :], sem.at[i]))
        copies[-1].start()
    wait(copies)


def pack_kernel(*refs):
    out = refs[-1]
    at = 0
    for r in refs[:-1]:
        out[:, at : at + r.shape[1]] = r[...]
        at += r.shape[1]


def cost(flops, read):
    return pl.CostEstimate(flops=int(flops), bytes_accessed=int(read), transcendentals=0)


def params(mib):
    return pltpu.CompilerParams(vmem_limit_bytes=mib * 1024 * 1024)


def rope_tables(first_row):
    half = HEAD // 2
    inverse = THETA ** (-jnp.arange(0, half, 2, dtype=F32) / half)
    count = EXT // GRID
    row = (first_row + jnp.arange(count, dtype=jnp.int32)).astype(F32)
    column = jnp.arange(GRID, dtype=jnp.int32).astype(F32)
    place = jnp.concatenate([row, column])
    angles = place[:, None] * jnp.concatenate([inverse] * 4)
    return jnp.cos(angles), jnp.sin(angles)


def body(
    tokens,
    query_weight,
    key_projection,
    value_projection,
    conv_in_weight,
    conv_gate_out,
    conv_gate_in,
    conv_taps,
    head_sink_logit,
    out_attn_weight,
    out_conv_weight,
    out_gain,
):
    s = lax.axis_index("sp")
    x = lax.axis_index("tp")
    z, core = s >> 3, s & 1
    sign = 2 * core - 1
    steps = jnp.array([0, 1, 2, 3, 4, -1, -2, -3], jnp.int32)
    plane_of = (z + sign * steps) & 7
    apart = (jnp.concatenate([plane_of, plane_of >> 1]) - x) & 3
    slot = jnp.where(apart == 3, 1, jnp.where(apart == 0, 0, apart + 1))
    sc = jnp.concatenate(
        [plane_of, jnp.full((8,), s, jnp.int32), slot[:8], 2 * slot[8:] + (plane_of & 1)]
    ).astype(jnp.int32)

    toks = x_pass(tokens, 1)
    last = ROWS - WINDOW
    within = lax.dynamic_slice(tokens, ((1 - core) * last, 0), (WINDOW, PART))
    across = lax.dynamic_slice(tokens, (core * last, 0), (WINDOW, PART))
    within = lax.ppermute(within, "sp", partner())
    across = lax.ppermute(across, "sp", next_chip())
    halos = x_pass(jnp.concatenate([within, across], 0), -1)
    stacked = jnp.concatenate([out_attn_weight.T, out_conv_weight.T], 1)
    stacked = lax.ppermute(stacked, ("sp", "tp"), spread_out_weights())

    packed = pl.pallas_call(
        pack_kernel,
        out_shape=jax.ShapeDtypeStruct((32, QKV + CNV + OUT), BF16),
        in_specs=[VMEM] * 7,
        out_specs=VMEM,
        cost_estimate=cost(1e6, 3e5),
    )(
        key_projection,
        value_projection,
        query_weight,
        conv_in_weight,
        conv_gate_in,
        conv_gate_out,
        stacked,
    )
    planes = [[chip(z, y, c) for y in range(4) for c in range(2)] for z in range(8)]
    plane = lax.all_gather(packed, "sp", axis=0, tiled=True, axis_index_groups=planes)
    w_qkv = z_ring(plane[:, :QKV])
    own_cnv = plane[:, QKV : QKV + CNV]
    w_cnv = z_ring(own_cnv)
    w_out = z_ring(plane[:, QKV + CNV :])

    cosine, sine = rope_tables(s * (ROWS // GRID) - WINDOW // GRID)

    mixer = jax.ShapeDtypeStruct((ROWS, 256), BF16)
    placed = pl.pallas_call(
        place_kernel,
        out_shape=jax.ShapeDtypeStruct((EXT, WIDTH), BF16),
        in_specs=[SMEM] + [ANY] * 8,
        out_specs=VMEM,
        scratch_shapes=[pltpu.SemaphoreType.DMA((12,))],
        compiler_params=params(8),
        cost_estimate=cost(1e6, 8e6),
    )(sc, *toks, *halos)
    kv, query = pl.pallas_call(
        project_kernel,
        out_shape=(jax.ShapeDtypeStruct((EXT, 256), BF16), mixer),
        in_specs=[SMEM] + [VMEM] * 11,
        out_specs=(VMEM,) * 2,
        compiler_params=params(16),
        cost_estimate=cost(2e9, 6e6),
    )(sc, placed, *w_qkv, cosine, sine)
    attention = pl.pallas_call(
        attn_kernel,
        out_shape=mixer,
        in_specs=[SMEM, SMEM] + [VMEM] * 2,
        out_specs=VMEM,
        compiler_params=params(10),
        cost_estimate=cost(2e9, 2e6),
    )(sc, head_sink_logit, kv, query)
    conv = pl.pallas_call(
        conv_kernel,
        out_shape=mixer,
        in_specs=[SMEM] + [VMEM] * 10,
        out_specs=VMEM,
        scratch_shapes=[pltpu.VMEM((CONV_ROWS, 256), F32)],
        compiler_params=params(18),
        cost_estimate=cost(3e9, 8e6),
    )(sc, placed, *w_cnv, conv_taps)
    attn_all = x_ring(attention)
    conv_all = x_ring(conv)
    partial, tail = pl.pallas_call(
        out_kernel,
        out_shape=(
            jax.ShapeDtypeStruct((ROWS, PART), F32),
            jax.ShapeDtypeStruct((PART, WIDTH - SOON), BF16),
        ),
        in_specs=[SMEM] + [ANY] * 16,
        out_specs=(VMEM, VMEM),
        scratch_shapes=[
            pltpu.VMEM((ROWS, WIDTH), BF16),
            pltpu.VMEM((PART, WIDTH), BF16),
            pltpu.SemaphoreType.DMA((24,)),
        ],
        compiler_params=params(16),
        cost_estimate=cost(1.4e9, 6e6),
    )(sc, *attn_all, *conv_all[:3], *w_out)
    summed, stats = pl.pallas_call(
        finish_kernel,
        out_shape=(
            jax.ShapeDtypeStruct((ROWS, PART), F32),
            jax.ShapeDtypeStruct((2, ROWS), F32),
        ),
        in_specs=[VMEM] * 4,
        out_specs=(VMEM, VMEM),
        compiler_params=params(14),
        cost_estimate=cost(4e8, 4e6),
    )(partial, tail, *conv_all[3:])
    others = []
    for d in (1, -1, 2):
        others.append(lax.ppermute(stats, "tp", turn(d)))
    return pl.pallas_call(
        norm_kernel,
        out_shape=jax.ShapeDtypeStruct((ROWS, PART), BF16),
        in_specs=[VMEM] * 6,
        out_specs=ANY,
        scratch_shapes=[
            pltpu.VMEM((ROWS, PART), BF16),
            pltpu.SemaphoreType.DMA((ROWS // 128,)),
        ],
        compiler_params=params(10),
        cost_estimate=cost(4e6, 3e6),
    )(summed, stats, *others, out_gain.reshape(1, PART))


def solution(mesh):
    return jax.shard_map(
        body,
        mesh=mesh,
        in_specs=(
            P("sp", "tp"),
            P("sp", "tp"),
            P("sp", "tp"),
            P("sp", "tp"),
            P("sp", "tp"),
            P("sp", "tp"),
            P("sp", "tp"),
            P(None, "tp"),
            P("tp"),
            P("tp", "sp"),
            P("tp", "sp"),
            P("tp"),
        ),
        out_specs=P("sp", "tp"),
        check_vma=False,
    )
```

```python
import jax
import jax.numpy as jnp
from jax import lax
from jax.experimental import pallas as pl
from jax.experimental.pallas import tpu as pltpu
from jax.sharding import PartitionSpec as P


HEAD = 128
WINDOW = 128
GRID = 64
NEG_BIG = -1e30
THETA = 10000.0
EPS = 1e-05

ROWS = 768
EXT = ROWS + 256
WIDTH = 2048
PART = 512
QKV = 512
CNV = 768
OUT = 512
ZB = 256


ANY = pl.BlockSpec(memory_space=pl.ANY)
SMEM = pl.BlockSpec(memory_space=pltpu.SMEM)
VMEM = pl.BlockSpec(memory_space=pltpu.VMEM)
F32 = jnp.float32
BF16 = jnp.bfloat16


def chip(z, y, c):
    return ((z % 8) * 4 + y % 4) * 2 + c


def up_down():
    return [
        (chip(z, y, c), chip(z + 1 - 2 * c, y, c))
        for z in range(8)
        for y in range(4)
        for c in range(2)
    ]


def partner():
    return [(i, i ^ 1) for i in range(64)]


def next_chip():
    return [(i, i + 1) for i in range(1, 63, 2)] + [(i, i - 1) for i in range(2, 64, 2)]


def turn(d):
    return [(i, (i + d) % 4) for i in range(4)]


def spread_out_weights():
    pairs = []
    for z in range(8):
        for y in range(4):
            for c in range(2):
                for t in range(4):
                    target = chip((z % 2) * 4 + t, y, c) * 4 + z // 2
                    pairs.append((chip(z, y, c) * 4 + t, target))
    return pairs


def x_ring(block):
    h = block.shape[0] // 2
    r1 = lax.ppermute(block, "tp", turn(1))
    l1 = lax.ppermute(block, "tp", turn(-1))
    r2 = lax.ppermute(r1[:h], "tp", turn(1))
    l2 = lax.ppermute(l1[h:], "tp", turn(-1))
    return [block, r1, l1, r2, l2]


def x_pass(block, way):
    r1 = lax.ppermute(block, "tp", turn(1))
    l1 = lax.ppermute(block, "tp", turn(-1))
    far = lax.ppermute(r1 if way == 1 else l1, "tp", turn(way))
    return [block, r1, l1, far]


def z_ring(block, joined=False):
    got, swapped = [block], []
    for _ in range(1, 5):
        got.append(lax.ppermute(got[-1], "sp", up_down()))
    if joined:
        return got + [lax.ppermute(jnp.concatenate(got[1:4], 0), "sp", partner())]
    for k in range(1, 4):
        swapped.append(lax.ppermute(got[k], "sp", partner()))
    return got + swapped


def start(copies):
    for c in copies:
        c.start()


def wait(copies):
    for c in copies:
        c.wait()


def place_kernel(sc, *refs):
    toks, halos, out, sem = refs[:4], refs[4:8], refs[8], refs[9]
    core = sc[8] & 1
    inner = pl.multiple_of((1 - core) * (EXT - WINDOW), WINDOW)
    outer = pl.multiple_of(core * (EXT - WINDOW), WINDOW)
    copies = []
    for i in range(4):
        lanes = slice(i * PART, (i + 1) * PART)
        spots = (
            (halos[i].at[:WINDOW, :], out.at[pl.ds(inner, WINDOW), lanes]),
            (toks[i], out.at[WINDOW : WINDOW + ROWS, lanes]),
            (halos[i].at[WINDOW:, :], out.at[pl.ds(outer, WINDOW), lanes]),
        )
        for j, (src, dst) in enumerate(spots):
            copies.append(pltpu.make_async_copy(src, dst, sem.at[3 * i + j]))
    start(copies)
    wait(copies)


def project(sc, tb, rows, ws, lanes):
    total = None
    for k, w in enumerate(ws):
        part = tb[rows, pl.ds(pl.multiple_of(sc[24 + k] * ZB, ZB), ZB)]
        part = jnp.dot(part, w[:, lanes], preferred_element_type=F32)
        total = part if total is None else total + part
    return total


def rotate(u, cos, sin, even):
    turned = jnp.where(even, -pltpu.roll(u, 96, 1), pltpu.roll(u, 32, 1))
    return u * cos + turned * sin


def spread_table(ref, first, count):
    by_row = lax.broadcasted_iota(jnp.int32, (GRID, HEAD), 1) < HEAD // 2
    column = ref[16 : 16 + GRID, :]
    groups = [
        jnp.where(by_row, jnp.broadcast_to(ref[pl.ds(first + g, 1), :], (GRID, HEAD)), column)
        for g in range(count)
    ]
    return jnp.concatenate(groups, 0)


def project_kernel(sc, tb, *refs):
    ws, (cos_ref, sin_ref, kv_ref, q_ref) = refs[:8], refs[8:]
    n = 256
    even = (lax.broadcasted_iota(jnp.int32, (n, HEAD), 1) // 32) % 2 == 0

    def keys(step, _):
        for i in (2 * step, 2 * step + 1):
            rows = pl.ds(pl.multiple_of(i * n, n), n)
            u = project(sc, tb, rows, ws, slice(0, 256))
            cos, sin = (spread_table(t, i * (n // GRID), n // GRID) for t in (cos_ref, sin_ref))
            kv_ref[rows, :HEAD] = rotate(u[:, :HEAD], cos, sin, even).astype(BF16)
            kv_ref[rows, HEAD:] = u[:, HEAD:].astype(BF16)
        return 0

    lax.fori_loop(0, EXT // (2 * n), keys, 0)

    def queries(i):
        rows = pl.ds(pl.multiple_of(i * n + WINDOW, WINDOW), n)
        u = project(sc, tb, rows, ws, slice(256, 512))
        place = i * (n // GRID) + WINDOW // GRID
        cos, sin = (spread_table(t, place, n // GRID) for t in (cos_ref, sin_ref))
        rows = pl.ds(pl.multiple_of(i * n, n), n)
        for h in range(2):
            lanes = slice(h * HEAD, (h + 1) * HEAD)
            q_ref[rows, lanes] = rotate(u[:, lanes], cos, sin, even).astype(BF16)

    for i in range(ROWS // n):
        queries(i)


def attn_kernel(sc, sink, kb, q_ref, out_ref):
    place = sc[12]
    two = 2 * WINDOW
    row = lax.broadcasted_iota(jnp.int32, (two, WINDOW), 0) % WINDOW
    col = lax.broadcasted_iota(jnp.int32, (two, WINDOW), 1)
    sinks = jnp.where(
        lax.broadcasted_iota(jnp.int32, (two, 1), 0) < WINDOW, sink[0], sink[1]
    )
    count = ROWS // WINDOW

    def block(n, left, right):
        first = pl.multiple_of(n * WINDOW, WINDOW)
        keys, rows = pl.ds(first, 3 * WINDOW), pl.ds(first, WINDOW)
        k, v = kb[keys, :HEAD], kb[keys, HEAD:]
        q = jnp.concatenate([q_ref[rows, :HEAD], q_ref[rows, HEAD:]], 0)
        s = lax.dot_general(q, k, (((1,), (1,)), ((), ())), preferred_element_type=F32)
        s = s * HEAD ** (-0.5)
        s0 = jnp.where(left, s[:, :WINDOW], NEG_BIG)
        s1 = s[:, WINDOW:two]
        s2 = jnp.where(right, s[:, two:], NEG_BIG)
        top = jnp.maximum(jnp.maximum(s0, s1), s2)
        top = jnp.maximum(jnp.max(top, -1, keepdims=True), sinks)
        w0, w1, w2 = jnp.exp(s0 - top), jnp.exp(s1 - top), jnp.exp(s2 - top)
        total = jnp.sum(w0 + w1 + w2, -1, keepdims=True) + jnp.exp(sinks - top)
        inverse = 1.0 / total
        probs = jnp.concatenate([w0 * inverse, w1 * inverse, w2 * inverse], 1).astype(BF16)
        o = jnp.dot(probs, v, preferred_element_type=F32).astype(BF16)
        out_ref[rows, :HEAD] = o[:WINDOW]
        out_ref[rows, HEAD:] = o[WINDOW:]

    def pair(i, _):
        for n in (2 * i, 2 * i + 1):
            left, right = col >= row, col <= row
            left = left & (col >= jnp.where((place == 0) & (n == 0), WINDOW, 0))
            right = right & (col < jnp.where((place == 63) & (n == count - 1), 0, WINDOW))
            block(n, left, right)
        return 0

    lax.fori_loop(0, count // 2, pair, 0)


CONV_ROWS = ROWS + 32


def conv_kernel(sc, tb, *refs):
    ws, (taps_ref, out_ref, sb) = refs[:8], refs[8:]
    for lo, hi in ((0, 272), (272, 544), (544, 800)):
        both = project(sc, tb, slice(lo + 112, hi + 112), ws, slice(0, 512))
        sb[lo:hi, :] = (both[:, 256:] * both[:, :256]).astype(BF16).astype(F32)
    taps = taps_ref[...].astype(F32)

    def mix(i):
        r = pl.multiple_of(i * 256, 256)
        rows = pl.ds(pl.multiple_of(r + WINDOW, WINDOW), 256)
        gate = project(sc, tb, rows, ws, slice(512, 768))
        s = sb[pl.ds(pl.multiple_of(r + 8, 8), 272), :]
        before = pltpu.roll(s, 1, 0)[8:264]
        after = pltpu.roll(s, 271, 0)[8:264]
        conv = before * taps[0:1] + s[8:264] * taps[1:2] + after * taps[2:3]
        out_ref[pl.ds(r, 256), :] = (gate * conv).astype(BF16)
        return 0

    for i in range(ROWS // 256):
        mix(i)


SOON = 1792


def mixer_spots(pieces, mb, lane):
    own, r1, l1, r2, l2 = pieces
    h = ROWS // 2
    return [
        (own, mb.at[:, lane : lane + 256]),
        (r1, mb.at[:, lane + 256 : lane + 512]),
        (l1, mb.at[:, lane + 512 : lane + 768]),
        (r2, mb.at[:h, lane + 768 : lane + 1024]),
        (l2, mb.at[h:, lane + 768 : lane + 1024]),
    ]


def out_kernel(sc, *refs):
    attn, conv, ws = refs[:5], refs[5:8], list(refs[8:13])
    ws += [refs[13].at[pl.ds(k * ZB, ZB), :] for k in range(3)]
    part_ref, tail_ref, mb, wb, sem = refs[14:]
    spots = []
    for k, src in enumerate(ws):
        row = pl.multiple_of((sc[k] // 4) * ZB, ZB)
        lane = pl.multiple_of(sc[16 + k] * 256, 256)
        spots.append((src.at[:, :256], wb.at[pl.ds(row, ZB), pl.ds(lane, 256)]))
        lane = pl.multiple_of(sc[16 + k] * 256 + 1024, 256)
        spots.append((src.at[:, 256:], wb.at[pl.ds(row, ZB), pl.ds(lane, 256)]))
    spots += mixer_spots(attn, mb, 0) + mixer_spots(conv + (None, None), mb, 1024)[:3]
    copies = [pltpu.make_async_copy(a, b, sem.at[i]) for i, (a, b) in enumerate(spots)]
    start(copies)
    wait(copies)
    for i in range(ROWS // 256):
        rows = slice(i * 256, i * 256 + 256)
        part_ref[rows, :] = lax.dot_general(
            mb[rows, :SOON], wb[:, :SOON], (((1,), (1,)), ((), ())), preferred_element_type=F32
        )
    tail_ref[...] = wb[:, SOON:]


def finish_kernel(part_ref, tail_ref, top_ref, bottom_ref, out_ref, stat_ref):
    h = ROWS // 2
    for i, ref in enumerate((top_ref, bottom_ref)):
        s = part_ref[i * h : i * h + h, :] + lax.dot_general(
            ref[...], tail_ref[...], (((1,), (1,)), ((), ())), preferred_element_type=F32
        )
        out_ref[i * h : i * h + h, :] = s
        mean = jnp.sum(s, -1, keepdims=True) * (1.0 / PART)
        d = s - mean
        second = jnp.sum(d * d, -1, keepdims=True)
        for j in range(h // 128):
            part = slice(j * 128, j * 128 + 128)
            rows = slice(i * h + j * 128, i * h + j * 128 + 128)
            stat_ref[0:1, rows] = jnp.broadcast_to(mean[part], (128, 128)).T[0:1]
            stat_ref[1:2, rows] = jnp.broadcast_to(second[part], (128, 128)).T[0:1]


def norm_kernel(sum_ref, s0, s1, s2, s3, gain_ref, out_ref, buf, sem):
    parts = (s0, s1, s2, s3)
    gain = gain_ref[...]

    copies = []
    for i in range(ROWS // 128):
        rows = slice(i * 128, i * 128 + 128)
        means = [p[0:1, rows] for p in parts]
        mean = (means[0] + means[1] + means[2] + means[3]) * 0.25
        second = sum(p[1:2, rows] for p in parts)
        second = second + PART * sum((m - mean) * (m - mean) for m in means)
        scale = lax.rsqrt(second * (1.0 / WIDTH) + EPS)
        mean = jnp.broadcast_to(mean, (128, 128)).T[:, 0:1]
        scale = jnp.broadcast_to(scale, (128, 128)).T[:, 0:1]
        buf[rows, :] = ((sum_ref[rows, :] - mean) * scale * gain).astype(BF16)
        copies.append(pltpu.make_async_copy(buf.at[rows, :], out_ref.at[rows, :], sem.at[i]))
        copies[-1].start()
    wait(copies)


def pack_kernel(*refs):
    out = refs[-1]
    at = 0
    for r in refs[:-1]:
        out[:, at : at + r.shape[1]] = r[...]
        at += r.shape[1]


def cost(flops, read):
    return pl.CostEstimate(flops=int(flops), bytes_accessed=int(read), transcendentals=0)


def params(mib):
    return pltpu.CompilerParams(vmem_limit_bytes=mib * 1024 * 1024)


def rope_tables(first_row):
    half = HEAD // 2
    inverse = THETA ** (-jnp.arange(0, half, 2, dtype=F32) / half)
    count = EXT // GRID
    row = (first_row + jnp.arange(count, dtype=jnp.int32)).astype(F32)
    column = jnp.arange(GRID, dtype=jnp.int32).astype(F32)
    place = jnp.concatenate([row, column])
    angles = place[:, None] * jnp.concatenate([inverse] * 4)
    return jnp.cos(angles), jnp.sin(angles)


def body(
    tokens,
    query_weight,
    key_projection,
    value_projection,
    conv_in_weight,
    conv_gate_out,
    conv_gate_in,
    conv_taps,
    head_sink_logit,
    out_attn_weight,
    out_conv_weight,
    out_gain,
):
    s = lax.axis_index("sp")
    x = lax.axis_index("tp")
    z, core = s >> 3, s & 1
    sign = 2 * core - 1
    steps = jnp.array([0, 1, 2, 3, 4, -1, -2, -3], jnp.int32)
    plane_of = (z + sign * steps) & 7
    apart = (jnp.concatenate([plane_of, plane_of >> 1]) - x) & 3
    slot = jnp.where(apart == 3, 1, jnp.where(apart == 0, 0, apart + 1))
    sc = jnp.concatenate(
        [plane_of, jnp.full((8,), s, jnp.int32), slot[:8], 2 * slot[8:] + (plane_of & 1)]
    ).astype(jnp.int32)

    toks = x_pass(tokens, 1)
    last = ROWS - WINDOW
    within = lax.dynamic_slice(tokens, ((1 - core) * last, 0), (WINDOW, PART))
    across = lax.dynamic_slice(tokens, (core * last, 0), (WINDOW, PART))
    within = lax.ppermute(within, "sp", partner())
    across = lax.ppermute(across, "sp", next_chip())
    halos = x_pass(jnp.concatenate([within, across], 0), -1)
    stacked = jnp.concatenate([out_attn_weight.T, out_conv_weight.T], 1)
    stacked = lax.ppermute(stacked, ("sp", "tp"), spread_out_weights())

    packed = pl.pallas_call(
        pack_kernel,
        out_shape=jax.ShapeDtypeStruct((32, QKV + CNV + OUT), BF16),
        in_specs=[VMEM] * 7,
        out_specs=VMEM,
        cost_estimate=cost(1e6, 3e5),
    )(
        key_projection,
        value_projection,
        query_weight,
        conv_in_weight,
        conv_gate_in,
        conv_gate_out,
        stacked,
    )
    planes = [[chip(z, y, c) for y in range(4) for c in range(2)] for z in range(8)]
    plane = lax.all_gather(packed, "sp", axis=0, tiled=True, axis_index_groups=planes)
    w_qkv = z_ring(plane[:, :QKV])
    own_cnv = plane[:, QKV : QKV + CNV]
    w_cnv = z_ring(own_cnv)
    w_out = z_ring(plane[:, QKV + CNV :], joined=True)

    cosine, sine = rope_tables(s * (ROWS // GRID) - WINDOW // GRID)

    mixer = jax.ShapeDtypeStruct((ROWS, 256), BF16)
    placed = pl.pallas_call(
        place_kernel,
        out_shape=jax.ShapeDtypeStruct((EXT, WIDTH), BF16),
        in_specs=[SMEM] + [ANY] * 8,
        out_specs=VMEM,
        scratch_shapes=[pltpu.SemaphoreType.DMA((12,))],
        compiler_params=params(8),
        cost_estimate=cost(1e6, 8e6),
    )(sc, *toks, *halos)
    kv, query = pl.pallas_call(
        project_kernel,
        out_shape=(jax.ShapeDtypeStruct((EXT, 256), BF16), mixer),
        in_specs=[SMEM] + [VMEM] * 11,
        out_specs=(VMEM,) * 2,
        compiler_params=params(16),
        cost_estimate=cost(2e9, 6e6),
    )(sc, placed, *w_qkv, cosine, sine)
    attention = pl.pallas_call(
        attn_kernel,
        out_shape=mixer,
        in_specs=[SMEM, SMEM] + [VMEM] * 2,
        out_specs=VMEM,
        compiler_params=params(10),
        cost_estimate=cost(2e9, 2e6),
    )(sc, head_sink_logit, kv, query)
    conv = pl.pallas_call(
        conv_kernel,
        out_shape=mixer,
        in_specs=[SMEM] + [VMEM] * 10,
        out_specs=VMEM,
        scratch_shapes=[pltpu.VMEM((CONV_ROWS, 256), F32)],
        compiler_params=params(18),
        cost_estimate=cost(3e9, 8e6),
    )(sc, placed, *w_cnv, conv_taps)
    attn_all = x_ring(attention)
    conv_all = x_ring(conv)
    partial, tail = pl.pallas_call(
        out_kernel,
        out_shape=(
            jax.ShapeDtypeStruct((ROWS, PART), F32),
            jax.ShapeDtypeStruct((PART, WIDTH - SOON), BF16),
        ),
        in_specs=[SMEM] + [ANY] * 14,
        out_specs=(VMEM, VMEM),
        scratch_shapes=[
            pltpu.VMEM((ROWS, WIDTH), BF16),
            pltpu.VMEM((PART, WIDTH), BF16),
            pltpu.SemaphoreType.DMA((24,)),
        ],
        compiler_params=params(16),
        cost_estimate=cost(1.4e9, 6e6),
    )(sc, *attn_all, *conv_all[:3], *w_out)
    summed, stats = pl.pallas_call(
        finish_kernel,
        out_shape=(
            jax.ShapeDtypeStruct((ROWS, PART), F32),
            jax.ShapeDtypeStruct((2, ROWS), F32),
        ),
        in_specs=[VMEM] * 4,
        out_specs=(VMEM, VMEM),
        compiler_params=params(14),
        cost_estimate=cost(4e8, 4e6),
    )(partial, tail, *conv_all[3:])
    others = []
    for d in (1, -1, 2):
        others.append(lax.ppermute(stats, "tp", turn(d)))
    return pl.pallas_call(
        norm_kernel,
        out_shape=jax.ShapeDtypeStruct((ROWS, PART), BF16),
        in_specs=[VMEM] * 6,
        out_specs=ANY,
        scratch_shapes=[
            pltpu.VMEM((ROWS, PART), BF16),
            pltpu.SemaphoreType.DMA((ROWS // 128,)),
        ],
        compiler_params=params(10),
        cost_estimate=cost(4e6, 3e6),
    )(summed, stats, *others, out_gain.reshape(1, PART))


def solution(mesh):
    return jax.shard_map(
        body,
        mesh=mesh,
        in_specs=(
            P("sp", "tp"),
            P("sp", "tp"),
            P("sp", "tp"),
            P("sp", "tp"),
            P("sp", "tp"),
            P("sp", "tp"),
            P("sp", "tp"),
            P(None, "tp"),
            P("tp"),
            P("tp", "sp"),
            P("tp", "sp"),
            P("tp"),
        ),
        out_specs=P("sp", "tp"),
        check_vma=False,
    )
```
